128 devices in a mesh: ep: 32 (over z, y, core), tp: 4 (over x).
Axes of the slice: x: 4, y: 4, z: 4, core: 2. Of those that a mesh axis runs over, the one named last changes fastest.
Arguments:
- conv_value: bfloat16 [49152, 2048], P(('ep', 'tp')), may hold values from -6 to 6
- conv_gate: bfloat16 [49152, 2048], P(('ep', 'tp')), may hold values from -6 to 6
- conv_taps: float32 [31, 2048], replicated, may hold values from -1 to 1
- conv_gain: float32 [2048], replicated, may hold values from 0.1 to 1.9
- conv_bias: float32 [2048], replicated, may hold values from -3 to 3
- conv_projection: bfloat16 [2048, 4096], P(None, 'tp'), may hold values from -0.125 to 0.125
- expert_input: bfloat16 [16384, 4096], P('ep'), may hold values from -6 to 6
- expert_gain: float32 [4096], replicated, may hold values from 0.1 to 1.9
- route_experts: int32 [16384, 2], P('ep'), may hold values from 0 to 31, all different within a row; in each aligned block of 128 rows (0 to 127, 128 to 255, ...) at most 16 rows name the same one
- group_gate: float32 [16384], P('ep'), may hold values from 0.3 to 1
- expert_gate: float32 [16384, 2], P('ep'), may hold values from 0.1 to 1
- gate_weight: bfloat16 [32, 4096, 1024], P('ep', None, 'tp'), may hold values from -0.09375 to 0.09375
- up_weight: bfloat16 [32, 4096, 1024], P('ep', None, 'tp'), may hold values from -0.09375 to 0.09375
- down_weight: bfloat16 [32, 1024, 4096], P('ep', None, 'tp'), may hold values from -0.1875 to 0.1875
Outputs:
- conv_out: bfloat16 [49152, 4096], P('ep', 'tp')
- expert_out: bfloat16 [16384, 4096], P('ep', 'tp')
The draws below stay inside these ranges and needn't reach their ends.
Inputs may be any that keep to these rules, and one draw needn't show every extreme that they name: `route_experts`: each row names 2 different experts; in each aligned block of 128 rows no expert is named more than 16 times, and in some blocks one expert is named exactly 16 times.
All inputs are finite; a program needn't handle non-finite values.
Results may differ from the reference program's by a relative error of at most 0.0071.
Values may be sent and summed in bfloat16 or wider, within the bound.
A program may use at most 128 MiB of HBM per device.

```python
import math
import jax
import jax.numpy as jnp
import numpy as np
from jax import lax

D = 4096
CONV = 2048
KERNEL = 31
HID = 1024
EXPERTS = 32
TOP = 2
MOE_DEV = 128
CAP = 16
SEQ = 49152
MOE_ROWS = 16384


def level_of(stream_key, shape, split, low, largest):
    level = 1.0
    for position, blocks in split:
        draws = jax.random.uniform(jax.random.fold_in(jax.random.fold_in(stream_key, 6), position), (blocks,), jnp.float32, low / len(split), largest / len(split))
        level = level * jnp.repeat(jnp.exp(draws), shape[position] // blocks).reshape((-1,) + (1,) * (len(shape) - 1 - position))
    return level


def assign_block(stream_key, own, number, rows, number_of, top, limit, slope):
    sequence = jax.random.permutation(stream_key, number_of)
    crowded, common = portions_of(number_of, rows * top, limit, slope, True), portions_of(number_of, rows * top, limit, slope, False)
    places = jnp.arange(number_of)

    def named(tallies, offset_by):
        used = int((tallies > 0).sum())
        fixed = max(1, used // 4)
        passed = fixed + (places - fixed + offset_by * (used - fixed)) % max(1, number_of - fixed)
        return jnp.zeros((number_of,), jnp.int32).at[sequence[jnp.where(places < fixed, places, passed)]].set(jnp.asarray(tallies, jnp.int32))

    tallies = jnp.where(number % 4 == 0, named(crowded, number // 4), named(common, number - number // 4 - 1))
    mixed = jax.random.permutation(jax.random.fold_in(own, 3), number_of)
    donor, sink = mixed[0:number_of // 2 * 2:2], mixed[1:number_of // 2 * 2:2]
    margin = jnp.minimum(tallies[donor] - 1, limit - tallies[sink]) // 2
    margin = jnp.where((donor == sequence[0]) | (sink == sequence[0]) | (tallies[sink] == 0), 0, jnp.maximum(margin, 0))
    passed = jax.random.randint(jax.random.fold_in(own, 4), (number_of // 2,), 0, 1 << 20) % (margin + 1)
    tallies = tallies.at[donor].add(-passed).at[sink].add(passed)
    items = jnp.searchsorted(jnp.cumsum(tallies), jnp.arange(rows * top), side="right").astype(jnp.int32)
    table = items.reshape(top, rows).T
    table = table[jax.random.permutation(jax.random.fold_in(own, 1), rows)]
    offset_by = jax.random.randint(jax.random.fold_in(own, 2), (rows, 1), 0, top)
    return jnp.take_along_axis(table, (jnp.arange(top)[None, :] + offset_by) % top, axis=1)


def portions_of(count, total, bound, lean, full):
    weights = [(1 << 20) // math.isqrt(grade ** lean) + 1 for grade in range(1, count + 1)]
    largest = bound if full else min(bound, max(-(-total // count), total * weights[0] // sum(weights)))
    least = 1 if total - largest >= count - 1 else 0
    holding, rest = [largest] + [least] * (count - 1), total - largest - least * (count - 1)
    while rest > 0:
        candidates = [i for i in range(1, count) if holding[i] < largest] or [i for i in range(1, count) if holding[i] < bound]
        whole, remaining = sum([weights[i] for i in candidates]), rest
        for i in candidates:
            more = min(bound - holding[i], max(1, remaining * weights[i] // whole), rest)
            holding[i] = holding[i] + more
            rest = rest - more
    return np.array(holding)


def normal_values(rng, shape, deviation, most, shards=(), kind=jnp.bfloat16):
    level = level_of(rng, shape, shards, -0.22, 0.18) if shards else 1.0
    values = jax.random.normal(rng, shape, jnp.float32) * deviation * level
    return jnp.minimum(jnp.maximum(values, -most), most).astype(kind)


def setup_inputs(seed: int = 0) -> dict:
    splits = jax.random.split(jax.random.key(seed), 15)
    conv_value = normal_values(splits[0], (SEQ, CONV), 1.0, 6.0, ((0, 128),))
    conv_gate = normal_values(splits[1], (SEQ, CONV), 1.0, 6.0, ((0, 128),))
    conv_taps = normal_values(splits[2], (KERNEL, CONV), KERNEL ** -0.5, 1.0, (), jnp.float32)
    conv_gain = jnp.clip(1.0 + 0.18 * jax.random.normal(splits[3], (CONV,), jnp.float32), 0.1, 1.9)
    conv_bias = normal_values(splits[4], (CONV,), 0.5, 3.0, (), jnp.float32)
    conv_projection = normal_values(splits[5], (CONV, D), CONV ** -0.5, 0.125, ((1, 4),))
    expert_input = normal_values(splits[6], (MOE_ROWS, D), 1.0, 6.0, ((0, 32),))
    expert_gain = jnp.clip(1.0 + 0.18 * jax.random.normal(splits[7], (D,), jnp.float32), 0.1, 1.9)
    route_experts_keys = jax.random.split(jax.random.fold_in(splits[8], 1), MOE_ROWS // MOE_DEV)
    route_experts_turns = jax.random.permutation(jax.random.fold_in(splits[8], 3), MOE_ROWS // MOE_DEV)
    route_experts = jax.vmap(lambda own, number: assign_block(jax.random.fold_in(splits[8], 2), own, number, MOE_DEV, EXPERTS, TOP, CAP, 2))(route_experts_keys, route_experts_turns).reshape((MOE_ROWS, TOP))
    group_gate = jnp.clip(0.3 + 0.7 * jax.random.uniform(splits[9], (MOE_ROWS,), jnp.float32) ** level_of(splits[9], (MOE_ROWS,), ((0, 32),), -0.2, 0.2), 0.3, 1.0)
    expert_gate = jnp.clip(jnp.exp(math.log(1.0) - 2.3025851 * jax.random.uniform(splits[10], (MOE_ROWS, TOP), jnp.float32) ** level_of(splits[10], (MOE_ROWS, TOP), ((0, 32),), -0.2, 0.2)), 0.1, 1.0)
    gate_weight = normal_values(splits[11], (EXPERTS, D, HID), D ** -0.5, 0.09375, ((0, 32), (2, 4)))
    up_weight = normal_values(splits[12], (EXPERTS, D, HID), D ** -0.5, 0.09375, ((0, 32), (2, 4)))
    down_weight = normal_values(splits[13], (EXPERTS, HID, D), HID ** -0.5, 0.1875, ((0, 32), (2, 4)))
    return dict(conv_value=conv_value, conv_gate=conv_gate, conv_taps=conv_taps, conv_gain=conv_gain, conv_bias=conv_bias, conv_projection=conv_projection, expert_input=expert_input, expert_gain=expert_gain, route_experts=route_experts, group_gate=group_gate, expert_gate=expert_gate, gate_weight=gate_weight, up_weight=up_weight, down_weight=down_weight)


epsilon = 1e-06

def root_mean_norm(values, gain):
    widened = values.astype(jnp.float32)
    inverse_rms = lax.rsqrt(lax.optimization_barrier(jnp.mean(widened * widened, axis=-1, keepdims=True)) + epsilon)
    return (widened * inverse_rms * gain).astype(jnp.bfloat16)

def reference(conv_value, conv_gate, conv_taps, conv_gain, conv_bias, conv_projection, expert_input, expert_gain, route_experts, group_gate, expert_gate, gate_weight, up_weight, down_weight):
    gated_rows = (conv_value.astype(jnp.float32) * jax.nn.sigmoid(conv_gate.astype(jnp.float32))).astype(jnp.bfloat16)
    reach_back = KERNEL - 1
    extended = jnp.concatenate([jnp.zeros((reach_back, CONV), jnp.bfloat16), gated_rows], axis=0)
    mixed_conv = jnp.zeros((SEQ, CONV), jnp.float32)
    for lag_step in range(KERNEL):
        window = lax.slice_in_dim(extended, reach_back - lag_step, reach_back - lag_step + SEQ, axis=0)
        mixed_conv = mixed_conv + conv_taps[lag_step] * window.astype(jnp.float32)
    center = mixed_conv - lax.optimization_barrier(jnp.mean(mixed_conv, axis=-1, keepdims=True))
    spread = lax.optimization_barrier(jnp.mean(center * center, axis=-1, keepdims=True))
    activated = jax.nn.silu(center * lax.rsqrt(spread + epsilon) * conv_gain + conv_bias).astype(jnp.bfloat16)
    conv_out = jnp.dot(activated, conv_projection, preferred_element_type=jnp.float32).astype(jnp.bfloat16)
    normed = root_mean_norm(expert_input, expert_gain)
    blocks = MOE_ROWS // MOE_DEV
    picked_experts = route_experts.reshape(blocks, MOE_DEV * TOP)
    onehot = (picked_experts[:, :, None] == jnp.arange(EXPERTS, dtype=jnp.int32)[None, None, :]).astype(jnp.int32)
    before = jnp.cumsum(onehot, axis=1) - onehot
    positions = lax.optimization_barrier(jnp.sum(before * onehot, axis=2)).astype(jnp.int32)
    block_index = jnp.arange(blocks, dtype=jnp.int32)[:, None]
    token_index = block_index * MOE_DEV + jnp.arange(MOE_DEV * TOP, dtype=jnp.int32)[None, :] // TOP
    column = block_index * CAP + positions
    route_share = group_gate[:, None] * expert_gate / lax.optimization_barrier(jnp.sum(expert_gate, axis=1, keepdims=True))
    route_share = route_share.reshape(blocks, MOE_DEV * TOP)
    source = jnp.full((EXPERTS, blocks * CAP), -1, jnp.int32).at[picked_experts, column].set(token_index)
    shares = jnp.zeros((EXPERTS, blocks * CAP), jnp.float32).at[picked_experts, column].set(route_share)

    def one_expert(running, packed):
        indices, slot_shares, gate_matrix, up_matrix, down_matrix = packed
        safe_index = jnp.maximum(indices, 0)
        taken_rows = jnp.take(normed, safe_index, axis=0)
        gate_part = jnp.dot(taken_rows, gate_matrix, preferred_element_type=jnp.float32)
        up_part = jnp.dot(taken_rows, up_matrix, preferred_element_type=jnp.float32)
        hidden = (jax.nn.silu(gate_part) * up_part).astype(jnp.bfloat16)
        result = jnp.dot(hidden, down_matrix, preferred_element_type=jnp.float32).astype(jnp.bfloat16)
        return (running.at[safe_index].add(slot_shares[:, None] * result.astype(jnp.float32)), None)
    running, _ = lax.scan(one_expert, jnp.zeros((MOE_ROWS, D), jnp.float32), (source, shares, gate_weight, up_weight, down_weight))
    return (conv_out, running.astype(jnp.bfloat16))
```

```python
import jax
import jax.numpy as jnp
from jax import lax
from jax.experimental import pallas as pl
from jax.experimental.pallas import tpu as pltpu
from jax.sharding import PartitionSpec as P

EXPERTS = 32
TOP = 2
MOE_DEV = 128
CAP = 16
D = 4096
HID_PART = 256
OUT_PART = 1024
EP_TP = ("ep", "tp")
MESH = pl.DeviceIdType.MESH
BF16 = jnp.bfloat16
F32 = jnp.float32

epsilon = 1e-06


def expert_kernel(
    rows_hbm,
    gain,
    route,
    share,
    gate_hbm,
    up_hbm,
    down_hbm,
    out,
    tokens,
    slots,
    arrived,
    w_gate,
    w_up,
    w_down,
    hidden,
    result,
    back,
    partial,
    landed,
    meta,
    acc_gate,
    acc_up,
    load_sem,
    z_send,
    z_recv,
    m_send,
    m_recv,
    y_send,
    y_recv,
    x_send,
    x_recv,
    h_send,
    h_recv,
    b_send,
    b_recv,
    p_send,
    p_recv,
):
    ep = lax.axis_index("ep")
    x = lax.axis_index("tp")
    z, y, c = ep // 8, (ep // 2) % 4, ep % 2

    def at(dz, dy, dc, dx):
        there = (((z + dz) % 4) * 4 + (y + dy) % 4) * 2 + (c + dc) % 2
        return (there, (x + dx) % 4)

    def remote(src, dst, send, recv, device):
        return pltpu.make_async_remote_copy(
            src_ref=src, dst_ref=dst, send_sem=send, recv_sem=recv, device_id=device, device_id_type=MESH
        )

    quarter = (x, (x + 1) % 4)

    raw = [
        pltpu.make_async_copy(
            rows_hbm.at[pl.ds(pl.multiple_of(quarter[i] * MOE_DEV, MOE_DEV), MOE_DEV)],
            slots.at[2, i],
            load_sem.at[i],
        )
        for i in range(2)
    ]
    weights = [
        pltpu.make_async_copy(gate_hbm.at[0], w_gate, load_sem.at[2]),
        pltpu.make_async_copy(up_hbm.at[0], w_up, load_sem.at[3]),
        pltpu.make_async_copy(down_hbm.at[0], w_down, load_sem.at[4]),
    ]
    for load in raw + weights:
        load.start()

    barrier = pltpu.get_barrier_semaphore()
    partners = [at(dz, 0, 0, 0) for dz in (1, 2, 3)]
    partners += [at(0, dy, dc, 0) for dy in range(4) for dc in range(2) if dy or dc]
    partners += [at(0, 0, 0, dx) for dx in (1, 2, 3)]
    for device in partners:
        pl.semaphore_signal(barrier, inc=1, device_id=device, device_id_type=MESH)

    lane = lax.broadcasted_iota(jnp.int32, (128, 128), 1)
    sub = lax.broadcasted_iota(jnp.int32, (128, 128), 0)
    earlier = jnp.where(sub < lane, 1.0, 0.0).astype(BF16)
    expert_row = lax.broadcasted_iota(jnp.int32, (EXPERTS, 128), 0)
    for q in range(4):
        first, second = route[q, 0:1, :], route[q, 1:2, :]
        hot0 = jnp.where(expert_row == first, 1.0, 0.0)
        hot1 = jnp.where(expert_row == second, 1.0, 0.0)
        before = jnp.dot((hot0 + hot1).astype(BF16), earlier, preferred_element_type=F32)
        pos0 = jnp.sum(before * hot0, axis=0, keepdims=True)
        pos1 = jnp.sum(before * hot1, axis=0, keepdims=True)
        meta[0, q, 0:1, :] = first.astype(F32) * CAP + pos0
        meta[0, q, 1:2, :] = second.astype(F32) * CAP + pos1
        meta[0, q, 2:4, :] = share[q]
        meta[0, q, 4:8, :] = jnp.zeros((4, 128), F32)

    for i in range(2):
        raw[i].wait()

        @pl.loop(0, 8)
        def _(t):
            r = pl.ds(pl.multiple_of(t * 16, 16), 16)
            wide = slots[2, i, r, :].astype(F32)
            inverse = lax.rsqrt(jnp.mean(wide * wide, axis=-1, keepdims=True) + epsilon)
            tokens[0, i, r, :] = (wide * inverse * gain[...]).astype(BF16)

    pl.semaphore_wait(barrier, len(partners))

    meta_copies = {
        dz: remote(meta.at[0], meta.at[dz], m_send.at[dz], m_recv.at[dz], at(dz, 0, 0, 0)) for dz in (1, 2, 3)
    }
    for dz in (1, 3, 2):
        meta_copies[dz].start()

    def z_copy(dz, i):
        if dz == 2:
            source, step = (1, 1) if i == 0 else (3, 3)
        else:
            source, step = 0, dz
        return remote(tokens.at[source, i], tokens.at[dz, i], z_send.at[dz, i], z_recv.at[dz, i], at(step, 0, 0, 0))

    for dz, i in ((1, 0), (3, 1), (1, 1), (3, 0)):
        z_copy(dz, i).start()

    plane = (z * 128).astype(F32)
    slot_row = lax.broadcasted_iota(jnp.int32, (128, 128), 0).astype(F32)

    def y_copy(dz, i, dy, dc):
        there = ((y + dy) % 4) * 2 + (c + dc) % 2
        k = dy * 2 + dc
        return remote(
            slots.at[dz, i, pl.ds(pl.multiple_of(there * CAP, CAP), CAP)],
            arrived.at[dz, k, quarter[i]],
            y_send.at[dz, i, k],
            y_recv.at[dz, i, k],
            at(0, dy, dc, 0),
        )

    y_order = [(0, 1), (1, 0), (3, 0), (1, 1), (3, 1), (2, 0), (2, 1)]

    def build(dz, i):
        q = quarter[i]
        hot = jnp.where(slot_row == meta[dz, q, 0:1, :] - plane, 1.0, 0.0)
        hot = hot + jnp.where(slot_row == meta[dz, q, 1:2, :] - plane, 1.0, 0.0)
        hot = hot.astype(BF16)

        @pl.loop(0, D // 512)
        def _(t):
            cols = pl.ds(pl.multiple_of(t * 512, 512), 512)
            slots[dz, i, :, cols] = jnp.dot(hot, tokens[dz, i, :, cols], preferred_element_type=F32).astype(BF16)

        for dy, dc in y_order:
            y_copy(dz, i, dy, dc).start()
        own = pl.ds(pl.multiple_of((y * 2 + c) * CAP, CAP), CAP)
        arrived[dz, 0, q] = slots[dz, i, own, :]

    def take_z(dz, i):
        z_copy(dz, i).wait_recv()

    def x_copy(dz, i, k):
        q = quarter[i]
        return remote(
            arrived.at[dz, k, q],
            arrived.at[dz, k, q],
            x_send.at[dz, i, k],
            x_recv.at[dz, i, k],
            at(0, 0, 0, 1 if i == 0 else 3),
        )

    def pass_on(dz, i):
        x_copy(dz, i, 0).start()
        for dy, dc in y_order:
            y_copy(dz, i, dy, dc).wait_recv()
            x_copy(dz, i, dy * 2 + dc).start()

    def x_landing(dz, i, k):
        q = (x + 3) % 4 if i == 0 else (x + 2) % 4
        return remote(
            arrived.at[dz, k, q],
            arrived.at[dz, k, q],
            x_send.at[dz, i, k],
            x_recv.at[dz, i, k],
            at(0, 0, 0, 3 if i == 0 else 1),
        )

    def h_copy(dz, dx):
        return remote(hidden.at[dz, x], hidden.at[dz, x], h_send.at[dz, dx], h_recv.at[dz, dx], at(0, 0, 0, dx))

    def h_landing(dz, dx):
        source = (x + 4 - dx) % 4
        return remote(
            hidden.at[dz, source], hidden.at[dz, source], h_send.at[dz, dx], h_recv.at[dz, dx], at(0, 0, 0, dx)
        )

    KB = 512

    def first_product(g):
        for i in range(2):
            for k in range(8):
                x_landing(g, i, k).wait_recv()
        acc_gate[...] = jnp.zeros_like(acc_gate)
        acc_up[...] = jnp.zeros_like(acc_up)

        @pl.loop(0, D // KB)
        def _(t):
            cols = pl.ds(pl.multiple_of(t * KB, KB), KB)
            piece = arrived[g, :, :, :, cols].reshape(512, KB)
            acc_gate[...] += jnp.dot(piece, w_gate[cols, :], preferred_element_type=F32)
            acc_up[...] += jnp.dot(piece, w_up[cols, :], preferred_element_type=F32)

        @pl.loop(0, 8)
        def _(t):
            r = pl.ds(pl.multiple_of(t * 64, 64), 64)
            gate = acc_gate[r, :]
            hidden[g, x, r, :] = (gate / (1.0 + jnp.exp(-gate)) * acc_up[r, :]).astype(BF16)

        for dx in (1, 3, 2):
            h_copy(g, dx).start()

    def b_copy(g, dy, dc):
        k = dy * 2 + dc
        return remote(
            result.at[g, k],
            back.at[g, :, y * 2 + c],
            b_send.at[g, k],
            b_recv.at[g, k],
            at(0, (4 - dy) % 4, dc, 0),
        )

    def b_landing(g, dy, dc):
        k = dy * 2 + dc
        source = ((y + dy) % 4) * 2 + (c + dc) % 2
        return remote(
            result.at[g, k],
            back.at[g, :, source],
            b_send.at[g, k],
            b_recv.at[g, k],
            at(0, (4 - dy) % 4, dc, 0),
        )

    def second_product(g):
        for dx in (1, 3, 2):
            h_landing(g, dx).wait_recv()

        @pl.loop(0, OUT_PART // 256)
        def _(t):
            cols = pl.ds(pl.multiple_of(t * 256, 256), 256)
            total = jnp.dot(hidden[g, 0], w_down[0:256, cols], preferred_element_type=F32)
            for s in range(1, 4):
                total += jnp.dot(hidden[g, s], w_down[s * 256 : (s + 1) * 256, cols], preferred_element_type=F32)
            result[g, :, :, :, cols] = total.astype(BF16).reshape(8, 4, CAP, 256)

        for dy, dc in y_order:
            b_copy(g, dy, dc).start()
        back[g, :, y * 2 + c] = result[g, 0]

    def p_copy(g):
        return remote(partial.at[g], landed.at[g - 1], p_send.at[g], p_recv.at[g], at(4 - g, 0, 0, 0))

    def combine(g):
        for dy, dc in y_order:
            b_landing(g, dy, dc).wait_recv()

        @pl.loop(0, 4)
        def _(q):
            weight = jnp.where(slot_row == meta[g, q, 0:1, :] - plane, meta[g, q, 2:3, :], 0.0)
            weight = weight + jnp.where(slot_row == meta[g, q, 1:2, :] - plane, meta[g, q, 3:4, :], 0.0)
            high = weight.astype(BF16)
            low = (weight - high.astype(F32)).astype(BF16)
            rows = back[g, q].reshape(128, OUT_PART)
            dims = (((0,), (0,)), ((), ()))
            total = lax.dot_general(high, rows, dims, preferred_element_type=F32)
            total += lax.dot_general(low, rows, dims, preferred_element_type=F32)
            partial[g, pl.ds(pl.multiple_of(q * 128, 128), 128), :] = total.astype(BF16)

        if g:
            p_copy(g).start()

    build(0, 0)
    build(0, 1)
    pass_on(0, 0)
    pass_on(0, 1)
    for load in weights:
        load.wait()
    meta_copies[1].wait_recv()
    meta_copies[3].wait_recv()
    take_z(1, 0)
    z_copy(2, 0).start()
    build(1, 0)
    take_z(3, 1)
    z_copy(2, 1).start()
    build(3, 1)
    pass_on(1, 0)
    pass_on(3, 1)
    first_product(0)
    take_z(1, 1)
    build(1, 1)
    take_z(3, 0)
    build(3, 0)
    pass_on(1, 1)
    pass_on(3, 0)
    second_product(0)
    meta_copies[2].wait_recv()
    take_z(2, 0)
    build(2, 0)
    take_z(2, 1)
    build(2, 1)
    first_product(1)
    pass_on(2, 0)
    pass_on(2, 1)
    first_product(3)
    second_product(1)
    combine(0)
    second_product(3)
    first_product(2)
    combine(1)
    combine(3)
    second_product(2)
    combine(2)

    for g in (1, 3, 2):
        p_copy(g).wait_recv()

    @pl.loop(0, 16)
    def _(t):
        r = pl.ds(pl.multiple_of(t * 32, 32), 32)
        total = partial[0, r, :].astype(F32) + landed[0, r, :].astype(F32)
        total = total + landed[1, r, :].astype(F32) + landed[2, r, :].astype(F32)
        out[r, :] = total.astype(BF16)

    for dz in (1, 2, 3):
        meta_copies[dz].wait_send()
        p_copy(dz).wait_send()
        for i in range(2):
            z_copy(dz, i).wait_send()
    for g in range(4):
        for dx in (1, 2, 3):
            h_copy(g, dx).wait_send()
        for dy, dc in y_order:
            b_copy(g, dy, dc).wait_send()
        for i in range(2):
            for k in range(8):
                x_copy(g, i, k).wait_send()
            for dy, dc in y_order:
                y_copy(g, i, dy, dc).wait_send()


def expert_branch(expert_input, expert_gain, route, share, gate_weight, up_weight, down_weight):
    vmem, hbm = pl.BlockSpec(memory_space=pltpu.VMEM), pl.BlockSpec(memory_space=pl.ANY)
    dma = pltpu.SemaphoreType.DMA
    return pl.pallas_call(
        expert_kernel,
        name="experts",
        out_shape=jax.ShapeDtypeStruct((512, OUT_PART), BF16),
        in_specs=[hbm, vmem, vmem, vmem, hbm, hbm, hbm],
        out_specs=vmem,
        scratch_shapes=[
            pltpu.VMEM((4, 2, 128, D), BF16),
            pltpu.VMEM((4, 2, 128, D), BF16),
            pltpu.VMEM((4, 8, 4, CAP, D), BF16),
            pltpu.VMEM((D, HID_PART), BF16),
            pltpu.VMEM((D, HID_PART), BF16),
            pltpu.VMEM((1024, OUT_PART), BF16),
            pltpu.VMEM((4, 4, 512, HID_PART), BF16),
            pltpu.VMEM((4, 8, 4, CAP, OUT_PART), BF16),
            pltpu.VMEM((4, 4, 8, CAP, OUT_PART), BF16),
            pltpu.VMEM((4, 512, OUT_PART), BF16),
            pltpu.VMEM((3, 512, OUT_PART), BF16),
            pltpu.VMEM((4, 4, 8, 128), F32),
            pltpu.VMEM((512, HID_PART), F32),
            pltpu.VMEM((512, HID_PART), F32),
            dma((5,)),
            dma((4, 2)),
            dma((4, 2)),
            dma((4,)),
            dma((4,)),
            dma((4, 2, 8)),
            dma((4, 2, 8)),
            dma((4, 2, 8)),
            dma((4, 2, 8)),
            dma((4, 4)),
            dma((4, 4)),
            dma((4, 8)),
            dma((4, 8)),
            dma((4,)),
            dma((4,)),
        ],
        compiler_params=pltpu.CompilerParams(
            collective_id=0, has_side_effects=True, vmem_limit_bytes=67_043_328
        ),
        cost_estimate=pl.CostEstimate(flops=150_000_000_000, bytes_accessed=16 << 20, transcendentals=0),
    )(expert_input, expert_gain, route, share, gate_weight, up_weight, down_weight)


def on_device(
    conv_value,
    conv_gate,
    conv_taps,
    conv_gain,
    conv_bias,
    conv_projection,
    expert_input,
    expert_gain,
    route_experts,
    group_gate,
    expert_gate,
    gate_weight,
    up_weight,
    down_weight,
):
    gated_rows = (
        conv_value.astype(jnp.float32) * jax.nn.sigmoid(conv_gate.astype(jnp.float32))
    ).astype(jnp.bfloat16)
    reach_back = conv_taps.shape[0] - 1
    length = gated_rows.shape[0]
    count = lax.axis_size(EP_TP)
    earlier = lax.ppermute(gated_rows[length - reach_back :], EP_TP, [(s, s + 1) for s in range(count - 1)])
    extended = jnp.concatenate([earlier, gated_rows], axis=0)
    mixed_conv = jnp.zeros(gated_rows.shape, jnp.float32)
    for lag_step in range(reach_back + 1):
        window = lax.slice_in_dim(
            extended, reach_back - lag_step, reach_back - lag_step + length, axis=0
        )
        mixed_conv = mixed_conv + conv_taps[lag_step] * window.astype(jnp.float32)
    center = mixed_conv - jnp.mean(mixed_conv, axis=-1, keepdims=True)
    spread = jnp.mean(center * center, axis=-1, keepdims=True)
    activated = jax.nn.silu(center * lax.rsqrt(spread + epsilon) * conv_gain + conv_bias).astype(
        jnp.bfloat16
    )

    route_share = group_gate[:, None] * expert_gate / jnp.sum(expert_gate, axis=1, keepdims=True)
    route = route_experts.reshape(4, MOE_DEV, TOP).transpose(0, 2, 1)
    share = route_share.reshape(4, MOE_DEV, TOP).transpose(0, 2, 1)
    activated, route, share = lax.optimization_barrier((activated, route, share))
    gathered = lax.all_gather(activated, "tp", axis=0, tiled=True)
    expert_out = expert_branch(
        expert_input, expert_gain[None], route, share, gate_weight, up_weight, down_weight
    )
    conv_out = jnp.dot(gathered, conv_projection, preferred_element_type=jnp.float32).astype(jnp.bfloat16)
    return (conv_out, expert_out)


def solution(mesh):
    in_specs = (
        P(EP_TP, None),
        P(EP_TP, None),
        P(),
        P(),
        P(),
        P(None, "tp"),
        P("ep", None),
        P(),
        P("ep", None),
        P("ep"),
        P("ep", None),
        P("ep", None, "tp"),
        P("ep", None, "tp"),
        P("ep", None, "tp"),
    )
    out_specs = (P("ep", "tp"), P("ep", "tp"))
    return jax.shard_map(
        on_device, mesh=mesh, in_specs=in_specs, out_specs=out_specs, check_vma=False
    )
```

```python
import jax
import jax.numpy as jnp
from jax import lax
from jax.experimental import pallas as pl
from jax.experimental.pallas import tpu as pltpu
from jax.sharding import PartitionSpec as P

EXPERTS = 32
TOP = 2
MOE_DEV = 128
CAP = 16
D = 4096
CONV = 2048
KERNEL = 31
ROWS = 384
HALO = 32
BLOCK = 128
HID_PART = 256
OUT_PART = 1024
EP_TP = ("ep", "tp")
MESH = pl.DeviceIdType.MESH
BF16 = jnp.bfloat16
F32 = jnp.float32

epsilon = 1e-06

BUFFER = {(0, 0): 0, (0, 1): 1, (1, 0): 2, (3, 1): 3, (1, 1): 4, (3, 0): 5, (2, 0): 0, (2, 1): 1}
RESULT = {0: 0, 1: 1, 3: 0, 2: 1}
PAIRS = [((0, 0), (0, 1)), ((1, 0), (3, 1)), ((3, 0), (1, 1)), ((2, 0), (2, 1))]
Y_ORDER = [(0, 1), (1, 0), (3, 0), (1, 1), (3, 1), (2, 0), (2, 1)]


def kernel(
    value_hbm,
    gate_rows_hbm,
    taps,
    conv_gain,
    conv_bias,
    projection_hbm,
    rows_hbm,
    gain,
    route,
    share,
    gate_hbm,
    up_hbm,
    down_hbm,
    conv_out,
    out_hbm,
    tokens,
    slots,
    arrived,
    w_gate,
    w_up,
    w_down,
    hidden,
    result,
    back,
    partial,
    landed,
    out,
    meta,
    acc_gate,
    acc_up,
    gated,
    mixed,
    w_conv,
    load_sem,
    z_send,
    z_recv,
    m_send,
    m_recv,
    y_send,
    y_recv,
    x_send,
    x_recv,
    h_send,
    h_recv,
    b_send,
    b_recv,
    p_send,
    p_recv,
    halo_sem,
    c_send,
    c_recv,
    store_sem,
    out_sem,
    free_sem,
):
    ep = lax.axis_index("ep")
    x = lax.axis_index("tp")
    z, y, c = ep // 8, (ep // 2) % 4, ep % 2

    def at(dz, dy, dc, dx):
        there = (((z + dz) % 4) * 4 + (y + dy) % 4) * 2 + (c + dc) % 2
        return (there, (x + dx) % 4)

    def remote(src, dst, send, recv, device):
        return pltpu.make_async_remote_copy(
            src_ref=src, dst_ref=dst, send_sem=send, recv_sem=recv, device_id=device, device_id_type=MESH
        )

    quarter = (x, (x + 1) % 4)
    number = ep * 4 + x
    after, ahead = (number + 1) % 128, (number + 127) % 128

    raw = [
        pltpu.make_async_copy(
            rows_hbm.at[pl.ds(pl.multiple_of(quarter[i] * MOE_DEV, MOE_DEV), MOE_DEV)],
            slots.at[2 + i],
            load_sem.at[i],
        )
        for i in range(2)
    ]
    value_load = pltpu.make_async_copy(value_hbm, gated.at[pl.ds(HALO, ROWS)], load_sem.at[2])
    gate_loads = [
        pltpu.make_async_copy(
            gate_rows_hbm.at[pl.ds(b * BLOCK, BLOCK)],
            slots.at[4 + b // 2, :, pl.ds((b % 2) * CONV, CONV)],
            load_sem.at[3 + b],
        )
        for b in range(3)
    ]
    weights = [
        pltpu.make_async_copy(gate_hbm.at[0], w_gate, load_sem.at[6]),
        pltpu.make_async_copy(up_hbm.at[0], w_up, load_sem.at[7]),
        pltpu.make_async_copy(down_hbm.at[0], w_down, load_sem.at[8]),
        pltpu.make_async_copy(projection_hbm, w_conv, load_sem.at[9]),
    ]
    for load in raw + [value_load] + gate_loads + weights:
        load.start()

    barrier = pltpu.get_barrier_semaphore()
    partners = [at(dz, 0, 0, 0) for dz in (1, 2, 3)]
    partners += [at(0, dy, dc, 0) for dy in range(4) for dc in range(2) if dy or dc]
    partners += [at(0, 0, 0, dx) for dx in (1, 2, 3)]
    partners += [(after // 4, after % 4), (ahead // 4, ahead % 4)]
    for device in partners:
        pl.semaphore_signal(barrier, inc=1, device_id=device, device_id_type=MESH)

    lane = lax.broadcasted_iota(jnp.int32, (128, 128), 1)
    sub = lax.broadcasted_iota(jnp.int32, (128, 128), 0)
    earlier = jnp.where(sub < lane, 1.0, 0.0).astype(BF16)
    expert_row = lax.broadcasted_iota(jnp.int32, (EXPERTS, 128), 0)
    for q in range(4):
        first, second = route[q, 0:1, :], route[q, 1:2, :]
        hot0 = jnp.where(expert_row == first, 1.0, 0.0)
        hot1 = jnp.where(expert_row == second, 1.0, 0.0)
        before = jnp.dot((hot0 + hot1).astype(BF16), earlier, preferred_element_type=F32)
        pos0 = jnp.sum(before * hot0, axis=0, keepdims=True)
        pos1 = jnp.sum(before * hot1, axis=0, keepdims=True)
        meta[0, q, 0:1, :] = first.astype(F32) * CAP + pos0
        meta[0, q, 1:2, :] = second.astype(F32) * CAP + pos1
        meta[0, q, 2:4, :] = share[q]
        meta[0, q, 4:8, :] = jnp.zeros((4, 128), F32)

    for i in range(2):
        raw[i].wait()

        @pl.loop(0, 8)
        def _(t):
            r = pl.ds(pl.multiple_of(t * 16, 16), 16)
            wide = slots[2 + i, r, :].astype(F32)
            inverse = lax.rsqrt(jnp.mean(wide * wide, axis=-1, keepdims=True) + epsilon)
            tokens[0, i, r, :] = (wide * inverse * gain[...]).astype(BF16)

    pl.semaphore_wait(barrier, len(partners))

    meta_copies = {
        dz: remote(meta.at[0], meta.at[dz], m_send.at[dz], m_recv.at[dz], at(dz, 0, 0, 0)) for dz in (1, 2, 3)
    }
    for dz in (1, 3, 2):
        meta_copies[dz].start()

    def z_copy(dz, i):
        if dz == 2:
            source, step = (1, 1) if i == 0 else (3, 3)
        else:
            source, step = 0, dz
        return remote(tokens.at[source, i], tokens.at[dz, i], z_send.at[dz, i], z_recv.at[dz, i], at(step, 0, 0, 0))

    for dz, i in ((1, 0), (3, 1), (1, 1), (3, 0)):
        z_copy(dz, i).start()

    plane = (z * 128).astype(F32)
    slot_row = lax.broadcasted_iota(jnp.int32, (128, 128), 0).astype(F32)

    def y_copy(dz, i, dy, dc):
        there = ((y + dy) % 4) * 2 + (c + dc) % 2
        k = dy * 2 + dc
        return remote(
            slots.at[BUFFER[dz, i], pl.ds(pl.multiple_of(there * CAP, CAP), CAP)],
            arrived.at[dz, k, quarter[i]],
            y_send.at[dz, i, k],
            y_recv.at[dz, i, k],
            at(0, dy, dc, 0),
        )

    def build(dz, i):
        q = quarter[i]
        if dz == 2:
            for dy, dc in Y_ORDER:
                y_copy(0, i, dy, dc).wait_send()
        hot = jnp.where(slot_row == meta[dz, q, 0:1, :] - plane, 1.0, 0.0)
        hot = hot + jnp.where(slot_row == meta[dz, q, 1:2, :] - plane, 1.0, 0.0)
        hot = hot.astype(BF16)

        @pl.loop(0, D // 512)
        def _(t):
            cols = pl.ds(pl.multiple_of(t * 512, 512), 512)
            slots[BUFFER[dz, i], :, cols] = jnp.dot(
                hot, tokens[dz, i, :, cols], preferred_element_type=F32
            ).astype(BF16)


    def send_slots(pair):
        for dy, dc in Y_ORDER:
            for dz, i in pair:
                y_copy(dz, i, dy, dc).start()
        own = pl.ds(pl.multiple_of((y * 2 + c) * CAP, CAP), CAP)
        for dz, i in pair:
            arrived[dz, 0, quarter[i]] = slots[BUFFER[dz, i], own, :]

    def take_z(dz, i):
        z_copy(dz, i).wait_recv()

    def x_copy(dz, i, k):
        q = quarter[i]
        return remote(
            arrived.at[dz, k, q],
            arrived.at[dz, k, q],
            x_send.at[dz, i, k],
            x_recv.at[dz, i, k],
            at(0, 0, 0, 1 if i == 0 else 3),
        )

    def pass_on(pair, between):
        for dz, i in pair:
            x_copy(dz, i, 0).start()
        for step, (dy, dc) in enumerate(Y_ORDER):
            for work in between.get(step, ()):
                work()
            for dz, i in pair:
                y_copy(dz, i, dy, dc).wait_recv()
                x_copy(dz, i, dy * 2 + dc).start()

    def x_landing(dz, i, k):
        q = (x + 3) % 4 if i == 0 else (x + 2) % 4
        return remote(
            arrived.at[dz, k, q],
            arrived.at[dz, k, q],
            x_send.at[dz, i, k],
            x_recv.at[dz, i, k],
            at(0, 0, 0, 3 if i == 0 else 1),
        )

    def h_copy(g, way, source):
        half = pl.ds(0, 512) if way < 2 else pl.ds((way - 2) * 256, 256)
        piece = hidden.at[g, source, half]
        return remote(
            piece, piece, h_send.at[g, way], h_recv.at[g, way], at(0, 0, 0, 1 if way % 2 == 0 else 3)
        )

    KB = 512

    def first_product(g):
        for i in range(2):
            for k in range(8):
                x_landing(g, i, k).wait_recv()
        acc_gate[...] = jnp.zeros_like(acc_gate)
        acc_up[...] = jnp.zeros_like(acc_up)

        @pl.loop(0, D // KB)
        def _(t):
            cols = pl.ds(pl.multiple_of(t * KB, KB), KB)
            piece = arrived[g, :, :, :, cols].reshape(512, KB)
            acc_gate[...] += jnp.dot(piece, w_gate[cols, :], preferred_element_type=F32)
            acc_up[...] += jnp.dot(piece, w_up[cols, :], preferred_element_type=F32)

        @pl.loop(0, 8)
        def _(t):
            r = pl.ds(pl.multiple_of(t * 64, 64), 64)
            gate = acc_gate[r, :]
            hidden[g, x, r, :] = (gate / (1.0 + jnp.exp(-gate)) * acc_up[r, :]).astype(BF16)

        for way in (0, 1):
            h_copy(g, way, x).start()

    def pass_hidden(g):
        h_copy(g, 0, (x + 3) % 4).wait_recv()
        h_copy(g, 2, (x + 3) % 4).start()
        h_copy(g, 1, (x + 1) % 4).wait_recv()
        h_copy(g, 3, (x + 1) % 4).start()

    def b_copy(g, dy, dc):
        k = dy * 2 + dc
        return remote(
            result.at[RESULT[g], k],
            back.at[g, :, y * 2 + c],
            b_send.at[g, k],
            b_recv.at[g, k],
            at(0, (4 - dy) % 4, dc, 0),
        )

    def b_landing(g, dy, dc):
        k = dy * 2 + dc
        source = ((y + dy) % 4) * 2 + (c + dc) % 2
        return remote(
            result.at[RESULT[g], k],
            back.at[g, :, source],
            b_send.at[g, k],
            b_recv.at[g, k],
            at(0, (4 - dy) % 4, dc, 0),
        )

    def second_product(g):
        for way in (2, 3):
            h_copy(g, way, (x + 2) % 4).wait_recv()
        if g >= 2:
            for dy, dc in Y_ORDER:
                b_copy(0 if g == 3 else 1, dy, dc).wait_send()

        @pl.loop(0, OUT_PART // 256)
        def _(t):
            cols = pl.ds(pl.multiple_of(t * 256, 256), 256)
            total = jnp.dot(hidden[g, 0], w_down[0:256, cols], preferred_element_type=F32)
            for s in range(1, 4):
                total += jnp.dot(hidden[g, s], w_down[s * 256 : (s + 1) * 256, cols], preferred_element_type=F32)
            result[RESULT[g], :, :, :, cols] = total.astype(BF16).reshape(8, 4, CAP, 256)

        for dy, dc in Y_ORDER:
            b_copy(g, dy, dc).start()
        back[g, :, y * 2 + c] = result[RESULT[g], 0]

    def p_copy(g):
        return remote(partial.at[g - 1], landed.at[g - 1], p_send.at[g], p_recv.at[g], at(4 - g, 0, 0, 0))

    def combine(g):
        for dy, dc in Y_ORDER:
            b_landing(g, dy, dc).wait_recv()

        @pl.loop(0, 4)
        def _(q):
            weight = jnp.where(slot_row == meta[g, q, 0:1, :] - plane, meta[g, q, 2:3, :], 0.0)
            weight = weight + jnp.where(slot_row == meta[g, q, 1:2, :] - plane, meta[g, q, 3:4, :], 0.0)
            high = weight.astype(BF16)
            low = (weight - high.astype(F32)).astype(BF16)
            rows = back[g, q].reshape(128, OUT_PART)
            dims = (((0,), (0,)), ((), ()))
            total = lax.dot_general(high, rows, dims, preferred_element_type=F32)
            total += lax.dot_general(low, rows, dims, preferred_element_type=F32)
            r = pl.ds(pl.multiple_of(q * 128, 128), 128)
            if g:
                partial[g - 1, r, :] = total.astype(BF16)
            else:
                out[r, :] = total.astype(BF16)

        if g:
            p_copy(g).start()

    def out_store(part):
        r = pl.ds(part * 128, 128)
        return pltpu.make_async_copy(out.at[r], out_hbm.at[r], out_sem.at[part])

    def final_sum():
        for g in (1, 3, 2):
            p_copy(g).wait_recv()
        for part in range(4):

            @pl.loop(0, 4)
            def _(t):
                r = pl.ds(pl.multiple_of(part * 128 + t * 32, 32), 32)
                total = out[r, :].astype(F32) + landed[0, r, :].astype(F32)
                total = total + landed[1, r, :].astype(F32) + landed[2, r, :].astype(F32)
                out[r, :] = total.astype(BF16)

            out_store(part).start()

    halo = remote(
        gated.at[pl.ds(ROWS, HALO)], gated.at[pl.ds(0, HALO)], halo_sem.at[0], halo_sem.at[1], (after // 4, after % 4)
    )

    def conv_gate():
        value_load.wait()
        for load in gate_loads:
            load.wait()
        for b in range(3):

            @pl.loop(0, BLOCK // 16)
            def _(t):
                r = pl.ds(pl.multiple_of(t * 16, 16), 16)
                to = pl.ds(pl.multiple_of(HALO + b * BLOCK + t * 16, 16), 16)
                gate = slots[4 + b // 2, r, (b % 2) * CONV : (b % 2 + 1) * CONV].astype(F32)
                gated[to, :] = (gated[to, :].astype(F32) / (1.0 + jnp.exp(-gate))).astype(BF16)

        halo.start()

    tile_row = lax.broadcasted_iota(jnp.int32, (8, 128), 0)

    def take_halo():
        halo.wait_recv()

        @pl.when(number == 0)
        def _():
            gated[0:HALO, :] = jnp.zeros((HALO, CONV), BF16)

    def conv_columns(b, half):
        @pl.loop(half * (CONV // 256), (half + 1) * (CONV // 256))
        def _(t):
            cols = pl.ds(pl.multiple_of(t * 128, 128), 128)
            tap = [jnp.broadcast_to(taps[j : j + 1, cols], (8, 128)) for j in range(KERNEL)]
            tiles = []
            last = None
            for n in range((HALO + BLOCK) // 16):
                pair = gated[b * BLOCK + n * 16 : b * BLOCK + (n + 1) * 16, cols].astype(F32)
                for half in (pair[0:8], pair[8:16]):
                    tiles.append(half)
                    count = len(tiles)
                    if count < 4:
                        continue
                    sums = []
                    for j in range(8):
                        total = tap[j] * tiles[count - 1]
                        for a in range(1, 4):
                            if 8 * a + j < KERNEL:
                                total = total + tap[8 * a + j] * tiles[count - 1 - a]
                        sums.append(total)
                    if count > 4:
                        total = sums[0]
                        for j in range(1, 8):
                            total = total + pltpu.roll(jnp.where(tile_row >= 8 - j, last[j], sums[j]), j, 0)
                        row = (count - 5) * 8
                        mixed[row : row + 8, cols] = total
                    last = sums

    def conv_norm(b):
        @pl.loop(0, BLOCK // 16)
        def _(t):
            r = pl.ds(pl.multiple_of(t * 16, 16), 16)
            wide = mixed[r, :]
            center = wide - jnp.mean(wide, axis=-1, keepdims=True)
            spread = jnp.mean(center * center, axis=-1, keepdims=True)
            unit = center * lax.rsqrt(spread + epsilon) * conv_gain[...] + conv_bias[...]
            to = pl.ds(pl.multiple_of(b * BLOCK + t * 16, 16), 16)
            gated[to, :] = (unit / (1.0 + jnp.exp(-unit))).astype(BF16)

    def held(source, b, start=0, rows=BLOCK):
        return tokens.at[source, b // 2, pl.ds(start, rows), pl.ds((b % 2) * CONV, CONV)]

    def c_copy(way, b):
        return remote(
            gated.at[pl.ds(b * BLOCK, BLOCK)],
            held(x, b),
            c_send.at[way, b],
            c_recv.at[way, b],
            at(0, 0, 0, 1 if way == 0 else 3),
        )

    def c_landing(way, b):
        place = held((x + 3) % 4 if way == 0 else (x + 1) % 4, b)
        return remote(place, place, c_send.at[way, b], c_recv.at[way, b], at(0, 0, 0, 1 if way == 0 else 3))

    def c_pass(way, part, source):
        place = held(source, way - 2) if part == 0 else held(source, 2, (way - 2) * 64, 64)
        return remote(place, place, c_send.at[way, part], c_recv.at[way, part], at(0, 0, 0, 1 if way == 2 else 3))

    def free_tokens():
        for dz in (1, 2, 3):
            for i in range(2):
                z_copy(dz, i).wait_send()
        for dx in (1, 2, 3):
            pl.semaphore_signal(free_sem, inc=1, device_id=at(0, 0, 0, dx), device_id_type=MESH)

    def conv_send():
        pl.semaphore_wait(free_sem, 3)
        for turn in range(3):
            for way in range(2):
                c_copy(way, ((0, 2, 1), (1, 2, 0))[way][turn]).start()

    def conv_pass():
        c_landing(0, 0).wait_recv()
        c_pass(2, 0, (x + 3) % 4).start()
        c_landing(1, 1).wait_recv()
        c_pass(3, 0, (x + 1) % 4).start()
        c_landing(0, 2).wait_recv()
        c_pass(2, 1, (x + 3) % 4).start()
        c_landing(1, 2).wait_recv()
        c_pass(3, 1, (x + 1) % 4).start()

    def staged(dx, b):
        n = 3 * dx + b
        return n // 4, pl.ds((n % 4) * OUT_PART, OUT_PART)

    def conv_store(dx, b):
        source = (x + dx) % 4
        buffer, cols = staged(dx, b)
        return pltpu.make_async_copy(
            slots.at[buffer, :, cols],
            conv_out.at[pl.ds(pl.multiple_of(source * ROWS + b * BLOCK, BLOCK), BLOCK)],
            store_sem.at[dx, b],
        )

    def conv_product(dx, blocks=(0, 1, 2)):
        source = (x + dx) % 4
        if dx == 3:
            c_landing(0, 1).wait_recv()
        if dx == 1:
            c_landing(1, 0).wait_recv()
        for b in blocks:
            if dx == 2:
                for way, part in (((2, 0),), ((3, 0),), ((2, 1), (3, 1)))[b]:
                    c_pass(way, part, source).wait_recv()
            buffer, _ = staged(dx, b)
            base = ((3 * dx + b) % 4) * OUT_PART

            @pl.loop(0, OUT_PART // 256)
            def _(t):
                cols = pl.ds(pl.multiple_of(t * 256, 256), 256)
                to = pl.ds(pl.multiple_of(base + t * 256, 256), 256)
                if dx:
                    block = tokens[source, b // 2, :, (b % 2) * CONV : (b % 2 + 1) * CONV]
                else:
                    block = gated[b * BLOCK : (b + 1) * BLOCK, :]
                slots[buffer, :, to] = jnp.dot(block, w_conv[:, cols], preferred_element_type=F32).astype(BF16)

            conv_store(dx, b).start()

    def y_left():
        for dz in range(1, 4):
            for i in range(2):
                for dy, dc in Y_ORDER:
                    y_copy(dz, i, dy, dc).wait_send()

    def drain():
        for dz in (1, 2, 3):
            meta_copies[dz].wait_send()
        halo.wait_send()
        for g in range(4):
            for way in range(4):
                h_copy(g, way, (x, x, (x + 3) % 4, (x + 1) % 4)[way]).wait_send()
            if g >= 2:
                for dy, dc in Y_ORDER:
                    b_copy(g, dy, dc).wait_send()
            for i in range(2):
                for k in range(8):
                    x_copy(g, i, k).wait_send()
        for way in range(2):
            for b in range(3):
                c_copy(way, b).wait_send()
        for dx in (0, 1, 3):
            for b in range(3):
                conv_store(dx, b).wait()

    def finish():
        for dz in (1, 2, 3):
            p_copy(dz).wait_send()
        for way in range(2):
            for part in range(2):
                c_pass(way + 2, part, (x + 3) % 4 if way == 0 else (x + 1) % 4).wait_send()
        for part in range(4):
            out_store(part).wait()
        for b in range(3):
            conv_store(2, b).wait()

    def build_pair(number):
        for dz, i in PAIRS[number]:
            if number:
                take_z(dz, i)
            if number == 1:
                z_copy(2, i).start()
        if number == 1:
            meta_copies[1].wait_recv()
            meta_copies[3].wait_recv()
        if number == 3:
            meta_copies[2].wait_recv()
        for dz, i in PAIRS[number]:
            build(dz, i)
        send_slots(PAIRS[number])

    def pass_pair(number, between):
        pass_on(PAIRS[number], between)

    def wait_weights():
        for load in weights:
            load.wait()

    build_pair(0)
    conv_gate()
    conv_work = {0: [], 1: [take_halo]}
    for b in range(3):
        conv_work.setdefault(2 * b + 1, []).append(lambda b=b: conv_columns(b, 0))
        conv_work.setdefault(2 * b + 2, []).append(lambda b=b: conv_columns(b, 1))
        conv_work[2 * b + 2].append(lambda b=b: conv_norm(b))
    pass_pair(0, conv_work)
    build_pair(1)
    pass_pair(1, {3: [wait_weights, lambda: first_product(0)]})
    build_pair(2)
    pass_pair(2, {5: [lambda: build_pair(3)]})
    pass_pair(
        3,
        {
            0: [lambda: pass_hidden(0)],
            1: [lambda: first_product(1)],
            2: [lambda: first_product(3)],
            3: [lambda: second_product(0)],
            5: [lambda: pass_hidden(1)],
            6: [lambda: pass_hidden(3)],
        },
    )
    free_tokens()
    second_product(1)
    second_product(3)
    combine(0)
    first_product(2)
    combine(1)
    pass_hidden(2)
    conv_send()
    combine(3)
    second_product(2)
    y_left()
    conv_product(0)
    combine(2)
    conv_pass()
    conv_product(3)
    conv_product(1)
    drain()
    final_sum()
    conv_product(2, (0, 1))
    conv_product(2, (2,))
    finish()


def both_branches(*operands):
    vmem, hbm = pl.BlockSpec(memory_space=pltpu.VMEM), pl.BlockSpec(memory_space=pl.ANY)
    dma = pltpu.SemaphoreType.DMA
    return pl.pallas_call(
        kernel,
        name="experts",
        out_shape=(
            jax.ShapeDtypeStruct((4 * ROWS, OUT_PART), BF16),
            jax.ShapeDtypeStruct((512, OUT_PART), BF16),
        ),
        in_specs=[hbm, hbm, vmem, vmem, vmem, hbm, hbm, vmem, vmem, vmem, hbm, hbm, hbm],
        out_specs=(hbm, hbm),
        scratch_shapes=[
            pltpu.VMEM((4, 2, 128, D), BF16),
            pltpu.VMEM((6, 128, D), BF16),
            pltpu.VMEM((4, 8, 4, CAP, D), BF16),
            pltpu.VMEM((D, HID_PART), BF16),
            pltpu.VMEM((D, HID_PART), BF16),
            pltpu.VMEM((1024, OUT_PART), BF16),
            pltpu.VMEM((4, 4, 512, HID_PART), BF16),
            pltpu.VMEM((2, 8, 4, CAP, OUT_PART), BF16),
            pltpu.VMEM((4, 4, 8, CAP, OUT_PART), BF16),
            pltpu.VMEM((3, 512, OUT_PART), BF16),
            pltpu.VMEM((3, 512, OUT_PART), BF16),
            pltpu.VMEM((512, OUT_PART), BF16),
            pltpu.VMEM((4, 4, 8, 128), F32),
            pltpu.VMEM((512, HID_PART), F32),
            pltpu.VMEM((512, HID_PART), F32),
            pltpu.VMEM((HALO + ROWS, CONV), BF16),
            pltpu.VMEM((BLOCK, CONV), F32),
            pltpu.VMEM((CONV, OUT_PART), BF16),
            dma((10,)),
            dma((4, 2)),
            dma((4, 2)),
            dma((4,)),
            dma((4,)),
            dma((4, 2, 8)),
            dma((4, 2, 8)),
            dma((4, 2, 8)),
            dma((4, 2, 8)),
            dma((4, 4)),
            dma((4, 4)),
            dma((4, 8)),
            dma((4, 8)),
            dma((4,)),
            dma((4,)),
            dma((2,)),
            dma((4, 3)),
            dma((4, 3)),
            dma((4, 3)),
            dma((4,)),
            pltpu.SemaphoreType.REGULAR,
        ],
        compiler_params=pltpu.CompilerParams(
            collective_id=0, has_side_effects=True, vmem_limit_bytes=67_043_328
        ),
        cost_estimate=pl.CostEstimate(flops=150_000_000_000, bytes_accessed=16 << 20, transcendentals=0),
    )(*operands)


def on_device(
    conv_value,
    conv_gate,
    conv_taps,
    conv_gain,
    conv_bias,
    conv_projection,
    expert_input,
    expert_gain,
    route_experts,
    group_gate,
    expert_gate,
    gate_weight,
    up_weight,
    down_weight,
):
    route_share = group_gate[:, None] * expert_gate / jnp.sum(expert_gate, axis=1, keepdims=True)
    route = route_experts.reshape(4, MOE_DEV, TOP).transpose(0, 2, 1)
    share = route_share.reshape(4, MOE_DEV, TOP).transpose(0, 2, 1)
    return both_branches(
        conv_value,
        conv_gate,
        conv_taps,
        conv_gain[None],
        conv_bias[None],
        conv_projection,
        expert_input,
        expert_gain[None],
        route,
        share,
        gate_weight,
        up_weight,
        down_weight,
    )


def solution(mesh):
    in_specs = (
        P(EP_TP, None),
        P(EP_TP, None),
        P(),
        P(),
        P(),
        P(None, "tp"),
        P("ep", None),
        P(),
        P("ep", None),
        P("ep"),
        P("ep", None),
        P("ep", None, "tp"),
        P("ep", None, "tp"),
        P("ep", None, "tp"),
    )
    out_specs = (P("ep", "tp"), P("ep", "tp"))
    return jax.shard_map(
        on_device, mesh=mesh, in_specs=in_specs, out_specs=out_specs, check_vma=False
    )
```

```python
import jax
import jax.numpy as jnp
from jax import lax
from jax.experimental import pallas as pl
from jax.experimental.pallas import tpu as pltpu
from jax.sharding import PartitionSpec as P

EXPERTS = 32
TOP = 2
MOE_DEV = 128
CAP = 16
D = 4096
CONV = 2048
KERNEL = 31
ROWS = 384
HALO = 32
BLOCK = 128
HID_PART = 256
OUT_PART = 1024
EP_TP = ("ep", "tp")
MESH = pl.DeviceIdType.MESH
BF16 = jnp.bfloat16
F32 = jnp.float32

epsilon = 1e-06

BUFFER = {(0, 0): 0, (0, 1): 1, (1, 0): 2, (3, 1): 3, (1, 1): 4, (3, 0): 5, (2, 0): 0, (2, 1): 1}
RESULT = {0: 0, 1: 1, 3: 0, 2: 1}
PAIRS = [((0, 0), (0, 1)), ((1, 0), (3, 1)), ((3, 0), (1, 1)), ((2, 0), (2, 1))]
Y_ORDER = [(0, 1), (1, 0), (3, 0), (1, 1), (3, 1), (2, 0), (2, 1)]


def kernel(
    value_hbm,
    gate_rows_hbm,
    taps,
    conv_gain,
    conv_bias,
    projection_hbm,
    rows_hbm,
    gain,
    route,
    group_gate,
    expert_gate,
    gate_hbm,
    up_hbm,
    down_hbm,
    conv_out,
    out_hbm,
    tokens,
    slots,
    arrived,
    w_gate,
    w_up,
    w_down,
    hidden,
    result,
    back,
    partial,
    landed,
    out,
    meta,
    acc_gate,
    acc_up,
    gated,
    mixed,
    w_conv,
    load_sem,
    z_send,
    z_recv,
    m_send,
    m_recv,
    y_send,
    y_recv,
    x_send,
    x_recv,
    h_send,
    h_recv,
    b_send,
    b_recv,
    p_send,
    p_recv,
    halo_sem,
    c_send,
    c_recv,
    store_sem,
    out_sem,
    free_sem,
):
    ep = lax.axis_index("ep")
    x = lax.axis_index("tp")
    z, y, c = ep // 8, (ep // 2) % 4, ep % 2

    def at(dz, dy, dc, dx):
        there = (((z + dz) % 4) * 4 + (y + dy) % 4) * 2 + (c + dc) % 2
        return (there, (x + dx) % 4)

    def remote(src, dst, send, recv, device):
        return pltpu.make_async_remote_copy(
            src_ref=src, dst_ref=dst, send_sem=send, recv_sem=recv, device_id=device, device_id_type=MESH
        )

    quarter = (x, (x + 1) % 4)
    number = ep * 4 + x
    after, ahead = (number + 1) % 128, (number + 127) % 128

    raw = [
        pltpu.make_async_copy(
            rows_hbm.at[pl.ds(pl.multiple_of(quarter[i] * MOE_DEV, MOE_DEV), MOE_DEV)],
            slots.at[2 + i],
            load_sem.at[i],
        )
        for i in range(2)
    ]
    value_load = pltpu.make_async_copy(value_hbm, gated.at[pl.ds(HALO, ROWS)], load_sem.at[2])
    gate_loads = [
        pltpu.make_async_copy(
            gate_rows_hbm.at[pl.ds(b * BLOCK, BLOCK)],
            slots.at[4 + b // 2, :, pl.ds((b % 2) * CONV, CONV)],
            load_sem.at[3 + b],
        )
        for b in range(3)
    ]
    weights = [
        pltpu.make_async_copy(gate_hbm.at[0], w_gate, load_sem.at[6]),
        pltpu.make_async_copy(up_hbm.at[0], w_up, load_sem.at[7]),
        pltpu.make_async_copy(down_hbm.at[0], w_down, load_sem.at[8]),
        pltpu.make_async_copy(projection_hbm, w_conv, load_sem.at[9]),
    ]
    for load in raw + [value_load] + gate_loads + weights:
        load.start()

    barrier = pltpu.get_barrier_semaphore()
    partners = [at(dz, 0, 0, 0) for dz in (1, 2, 3)]
    partners += [at(0, dy, dc, 0) for dy in range(4) for dc in range(2) if dy or dc]
    partners += [at(0, 0, 0, dx) for dx in (1, 2, 3)]
    partners += [(after // 4, after % 4), (ahead // 4, ahead % 4)]
    for device in partners:
        pl.semaphore_signal(barrier, inc=1, device_id=device, device_id_type=MESH)

    lane = lax.broadcasted_iota(jnp.int32, (128, 128), 1)
    sub = lax.broadcasted_iota(jnp.int32, (128, 128), 0)
    earlier = jnp.where(sub < lane, 1.0, 0.0).astype(BF16)
    expert_row = lax.broadcasted_iota(jnp.int32, (EXPERTS, 128), 0)
    for q in range(4):
        lanes = slice(q * MOE_DEV, (q + 1) * MOE_DEV)
        first, second = route[0:1, lanes], route[1:2, lanes]
        gates = expert_gate[:, lanes]
        hot0 = jnp.where(expert_row == first, 1.0, 0.0)
        hot1 = jnp.where(expert_row == second, 1.0, 0.0)
        before = jnp.dot((hot0 + hot1).astype(BF16), earlier, preferred_element_type=F32)
        pos0 = jnp.sum(before * hot0, axis=0, keepdims=True)
        pos1 = jnp.sum(before * hot1, axis=0, keepdims=True)
        meta[0, q, 0:1, :] = first.astype(F32) * CAP + pos0
        meta[0, q, 1:2, :] = second.astype(F32) * CAP + pos1
        meta[0, q, 2:4, :] = group_gate[:, lanes] * gates / jnp.sum(gates, axis=0, keepdims=True)
        meta[0, q, 4:8, :] = jnp.zeros((4, 128), F32)

    for i in range(2):
        raw[i].wait()

        @pl.loop(0, 8)
        def _(t):
            r = pl.ds(pl.multiple_of(t * 16, 16), 16)
            wide = slots[2 + i, r, :].astype(F32)
            inverse = lax.rsqrt(jnp.mean(wide * wide, axis=-1, keepdims=True) + epsilon)
            tokens[0, i, r, :] = (wide * inverse * gain[...]).astype(BF16)

    pl.semaphore_wait(barrier, len(partners))

    meta_copies = {
        dz: remote(meta.at[0], meta.at[dz], m_send.at[dz], m_recv.at[dz], at(dz, 0, 0, 0)) for dz in (1, 2, 3)
    }
    for dz in (1, 3, 2):
        meta_copies[dz].start()

    def z_copy(dz, i):
        if dz == 2:
            source, step = (1, 1) if i == 0 else (3, 3)
        else:
            source, step = 0, dz
        return remote(tokens.at[source, i], tokens.at[dz, i], z_send.at[dz, i], z_recv.at[dz, i], at(step, 0, 0, 0))

    for dz, i in ((1, 0), (3, 1), (1, 1), (3, 0)):
        z_copy(dz, i).start()

    plane = (z * 128).astype(F32)
    slot_row = lax.broadcasted_iota(jnp.int32, (128, 128), 0).astype(F32)

    def y_copy(dz, i, dy, dc):
        there = ((y + dy) % 4) * 2 + (c + dc) % 2
        k = dy * 2 + dc
        return remote(
            slots.at[BUFFER[dz, i], pl.ds(pl.multiple_of(there * CAP, CAP), CAP)],
            arrived.at[dz, k, quarter[i]],
            y_send.at[dz, i],
            y_recv.at[dz, i, k],
            at(0, dy, dc, 0),
        )

    def y_left(dz, i):
        sent = slots.at[BUFFER[dz, i], pl.ds(0, 7 * CAP)]
        remote(sent, sent, y_send.at[dz, i], y_recv.at[dz, i, 0], at(0, 1, 0, 0)).wait_send()

    def build(dz, i):
        q = quarter[i]
        if dz == 2:
            y_left(0, i)
        hot = jnp.where(slot_row == meta[dz, q, 0:1, :] - plane, 1.0, 0.0)
        hot = hot + jnp.where(slot_row == meta[dz, q, 1:2, :] - plane, 1.0, 0.0)
        hot = hot.astype(BF16)

        @pl.loop(0, D // 512)
        def _(t):
            cols = pl.ds(pl.multiple_of(t * 512, 512), 512)
            slots[BUFFER[dz, i], :, cols] = jnp.dot(
                hot, tokens[dz, i, :, cols], preferred_element_type=F32
            ).astype(BF16)


    def send_slots(pair):
        for dy, dc in Y_ORDER:
            for dz, i in pair:
                y_copy(dz, i, dy, dc).start()
        own = pl.ds(pl.multiple_of((y * 2 + c) * CAP, CAP), CAP)
        for dz, i in pair:
            arrived[dz, 0, quarter[i]] = slots[BUFFER[dz, i], own, :]

    def take_z(dz, i):
        z_copy(dz, i).wait_recv()

    def x_copy(dz, i, k):
        q = quarter[i]
        return remote(
            arrived.at[dz, k, q],
            arrived.at[dz, k, q],
            x_send.at[dz, i],
            x_recv.at[dz, i],
            at(0, 0, 0, 1 if i == 0 else 3),
        )

    def pass_on(pair, between):
        for dz, i in pair:
            x_copy(dz, i, 0).start()
        for step, (dy, dc) in enumerate(Y_ORDER):
            for work in between.get(step, ()):
                work()
            for dz, i in pair:
                y_copy(dz, i, dy, dc).wait_recv()
                x_copy(dz, i, dy * 2 + dc).start()

    def x_all(dz, i, q):
        place = arrived.at[dz, :, q]
        return remote(place, place, x_send.at[dz, i], x_recv.at[dz, i], at(0, 0, 0, 3 if i == 0 else 1))

    def x_landed(dz, i):
        x_all(dz, i, (x + 3) % 4 if i == 0 else (x + 2) % 4).wait_recv()

    def x_left(dz, i):
        x_all(dz, i, quarter[i]).wait_send()

    def h_copy(g, way, source):
        half = pl.ds(0, 512) if way < 2 else pl.ds((way - 2) * 256, 256)
        piece = hidden.at[g, source, half]
        return remote(
            piece, piece, h_send.at[g], h_recv.at[g, way], at(0, 0, 0, 1 if way % 2 == 0 else 3)
        )

    KB = 512

    def first_product(g):
        for i in range(2):
            x_landed(g, i)
        acc_gate[...] = jnp.zeros_like(acc_gate)
        acc_up[...] = jnp.zeros_like(acc_up)

        @pl.loop(0, D // KB)
        def _(t):
            cols = pl.ds(pl.multiple_of(t * KB, KB), KB)
            piece = arrived[g, :, :, :, cols].reshape(512, KB)
            acc_gate[...] += jnp.dot(piece, w_gate[cols, :], preferred_element_type=F32)
            acc_up[...] += jnp.dot(piece, w_up[cols, :], preferred_element_type=F32)

        @pl.loop(0, 8)
        def _(t):
            r = pl.ds(pl.multiple_of(t * 64, 64), 64)
            gate = acc_gate[r, :]
            hidden[g, x, r, :] = (gate / (1.0 + jnp.exp(-gate)) * acc_up[r, :]).astype(BF16)

        for way in (0, 1):
            h_copy(g, way, x).start()

    def pass_hidden(g):
        h_copy(g, 0, (x + 3) % 4).wait_recv()
        h_copy(g, 2, (x + 3) % 4).start()
        h_copy(g, 1, (x + 1) % 4).wait_recv()
        h_copy(g, 3, (x + 1) % 4).start()

    def b_copy(g, dy, dc, half):
        pick = pl.ds(half * 2, 2)
        return remote(
            result.at[RESULT[g], dy * 2 + dc, pick],
            back.at[g, pick, y * 2 + c],
            b_send.at[g],
            b_recv.at[g, half],
            at(0, (4 - dy) % 4, dc, 0),
        )

    def b_left(g):
        sent = result.at[RESULT[g], pl.ds(1, 7)]
        remote(sent, sent, b_send.at[g], b_recv.at[g, 0], at(0, 1, 0, 0)).wait_send()

    def b_landed(g, half):
        place = result.at[RESULT[g], pl.ds(1, 7), pl.ds(0, 2)]
        remote(place, place, b_send.at[g], b_recv.at[g, half], at(0, 1, 0, 0)).wait_recv()

    def second_product(g):
        for way in (2, 3):
            h_copy(g, way, (x + 2) % 4).wait_recv()
        if g >= 2:
            b_left(0 if g == 3 else 1)

        @pl.loop(0, OUT_PART // 256)
        def _(t):
            cols = pl.ds(pl.multiple_of(t * 256, 256), 256)
            total = jnp.dot(hidden[g, 0], w_down[0:256, cols], preferred_element_type=F32)
            for s in range(1, 4):
                total += jnp.dot(hidden[g, s], w_down[s * 256 : (s + 1) * 256, cols], preferred_element_type=F32)
            result[RESULT[g], :, :, :, cols] = total.astype(BF16).reshape(8, 4, CAP, 256)

        for half in range(2):
            for dy, dc in Y_ORDER:
                b_copy(g, dy, dc, half).start()
        back[g, :, y * 2 + c] = result[RESULT[g], 0]

    def p_copy(g, half):
        r = pl.ds(half * 256, 256)
        return remote(
            partial.at[g - 1, r], landed.at[g - 1, r], p_send.at[g], p_recv.at[g, half], at(4 - g, 0, 0, 0)
        )

    def p_left(g):
        sent = partial.at[g - 1]
        remote(sent, sent, p_send.at[g], p_recv.at[g, 0], at(1, 0, 0, 0)).wait_send()

    def combine(g):
        for half in range(2):
            b_landed(g, half)

            @pl.loop(half * 2, half * 2 + 2)
            def _(q):
                weight = jnp.where(slot_row == meta[g, q, 0:1, :] - plane, meta[g, q, 2:3, :], 0.0)
                weight = weight + jnp.where(slot_row == meta[g, q, 1:2, :] - plane, meta[g, q, 3:4, :], 0.0)
                high = weight.astype(BF16)
                low = (weight - high.astype(F32)).astype(BF16)
                rows = back[g, q].reshape(128, OUT_PART)
                dims = (((0,), (0,)), ((), ()))
                total = lax.dot_general(high, rows, dims, preferred_element_type=F32)
                total += lax.dot_general(low, rows, dims, preferred_element_type=F32)
                r = pl.ds(pl.multiple_of(q * 128, 128), 128)
                if g:
                    partial[g - 1, r, :] = total.astype(BF16)
                else:
                    out[r, :] = total.astype(BF16)

            if g:
                p_copy(g, half).start()

    def out_store(part):
        r = pl.ds(part * 128, 128)
        return pltpu.make_async_copy(out.at[r], out_hbm.at[r], out_sem)

    def final_sum():
        for part in range(4):
            if part % 2 == 0:
                for g in (1, 3, 2):
                    p_copy(g, part // 2).wait_recv()

            @pl.loop(0, 4)
            def _(t):
                r = pl.ds(pl.multiple_of(part * 128 + t * 32, 32), 32)
                total = out[r, :].astype(F32) + landed[0, r, :].astype(F32)
                total = total + landed[1, r, :].astype(F32) + landed[2, r, :].astype(F32)
                out[r, :] = total.astype(BF16)

            out_store(part).start()

    halo = remote(
        gated.at[pl.ds(ROWS, HALO)], gated.at[pl.ds(0, HALO)], halo_sem.at[0], halo_sem.at[1], (after // 4, after % 4)
    )

    def conv_gate():
        value_load.wait()
        for load in gate_loads:
            load.wait()
        for b in range(3):

            @pl.loop(0, BLOCK // 16)
            def _(t):
                r = pl.ds(pl.multiple_of(t * 16, 16), 16)
                to = pl.ds(pl.multiple_of(HALO + b * BLOCK + t * 16, 16), 16)
                gate = slots[4 + b // 2, r, (b % 2) * CONV : (b % 2 + 1) * CONV].astype(F32)
                gated[to, :] = (gated[to, :].astype(F32) / (1.0 + jnp.exp(-gate))).astype(BF16)

        halo.start()

    tile_row = lax.broadcasted_iota(jnp.int32, (8, 128), 0)

    def take_halo():
        halo.wait_recv()

        @pl.when(number == 0)
        def _():
            gated[0:HALO, :] = jnp.zeros((HALO, CONV), BF16)

    def conv_columns(b, half):
        @pl.loop(half * (CONV // 256), (half + 1) * (CONV // 256))
        def _(t):
            cols = pl.ds(pl.multiple_of(t * 128, 128), 128)
            tap = [jnp.broadcast_to(taps[j : j + 1, cols], (8, 128)) for j in range(KERNEL)]
            tiles = []
            last = None
            for n in range((HALO + BLOCK) // 16):
                pair = gated[b * BLOCK + n * 16 : b * BLOCK + (n + 1) * 16, cols].astype(F32)
                for half in (pair[0:8], pair[8:16]):
                    tiles.append(half)
                    count = len(tiles)
                    if count < 4:
                        continue
                    sums = []
                    for j in range(8):
                        total = tap[j] * tiles[count - 1]
                        for a in range(1, 4):
                            if 8 * a + j < KERNEL:
                                total = total + tap[8 * a + j] * tiles[count - 1 - a]
                        sums.append(total)
                    if count > 4:
                        total = sums[0]
                        for j in range(1, 8):
                            total = total + pltpu.roll(jnp.where(tile_row >= 8 - j, last[j], sums[j]), j, 0)
                        row = (count - 5) * 8
                        mixed[row : row + 8, cols] = total
                    last = sums

    def conv_norm(b):
        @pl.loop(0, BLOCK // 16)
        def _(t):
            r = pl.ds(pl.multiple_of(t * 16, 16), 16)
            wide = mixed[r, :]
            center = wide - jnp.mean(wide, axis=-1, keepdims=True)
            spread = jnp.mean(center * center, axis=-1, keepdims=True)
            unit = center * lax.rsqrt(spread + epsilon) * conv_gain[...] + conv_bias[...]
            to = pl.ds(pl.multiple_of(b * BLOCK + t * 16, 16), 16)
            gated[to, :] = (unit / (1.0 + jnp.exp(-unit))).astype(BF16)

    def held(source, b, start=0, rows=BLOCK):
        return tokens.at[source, b // 2, pl.ds(start, rows), pl.ds((b % 2) * CONV, CONV)]

    def c_copy(way, b):
        return remote(
            gated.at[pl.ds(b * BLOCK, BLOCK)],
            held(x, b),
            c_send.at[way],
            c_recv.at[way, b],
            at(0, 0, 0, 1 if way == 0 else 3),
        )

    def c_landing(way, b):
        place = held((x + 3) % 4 if way == 0 else (x + 1) % 4, b)
        return remote(place, place, c_send.at[way], c_recv.at[way, b], at(0, 0, 0, 1 if way == 0 else 3))

    def c_pass(way, part, source):
        place = held(source, way - 2) if part == 0 else held(source, 2, (way - 2) * 64, 64)
        return remote(place, place, c_send.at[way], c_recv.at[way, part], at(0, 0, 0, 1 if way == 2 else 3))

    def c_left(way, rows):
        sent = gated.at[pl.ds(0, rows)]
        remote(sent, sent, c_send.at[way], c_recv.at[way, 0], at(0, 0, 0, 1)).wait_send()

    def free_tokens():
        for dz in (1, 2, 3):
            for i in range(2):
                z_copy(dz, i).wait_send()
        for dx in (1, 2, 3):
            pl.semaphore_signal(free_sem, inc=1, device_id=at(0, 0, 0, dx), device_id_type=MESH)

    def conv_send():
        pl.semaphore_wait(free_sem, 3)
        for turn in range(3):
            for way in range(2):
                c_copy(way, ((0, 2, 1), (1, 2, 0))[way][turn]).start()

    def conv_pass():
        c_landing(0, 0).wait_recv()
        c_pass(2, 0, (x + 3) % 4).start()
        c_landing(1, 1).wait_recv()
        c_pass(3, 0, (x + 1) % 4).start()
        c_landing(0, 2).wait_recv()
        c_pass(2, 1, (x + 3) % 4).start()
        c_landing(1, 2).wait_recv()
        c_pass(3, 1, (x + 1) % 4).start()

    def staged(dx, b):
        n = 3 * dx + b
        return n // 4, pl.ds((n % 4) * OUT_PART, OUT_PART)

    def conv_store(dx, b):
        source = (x + dx) % 4
        buffer, cols = staged(dx, b)
        return pltpu.make_async_copy(
            slots.at[buffer, :, cols],
            conv_out.at[pl.ds(pl.multiple_of(source * ROWS + b * BLOCK, BLOCK), BLOCK)],
            store_sem.at[dx],
        )

    def conv_stored(dx):
        rows = conv_out.at[pl.ds(0, ROWS)]
        pltpu.make_async_copy(rows, rows, store_sem.at[dx]).wait()

    def conv_product(dx, blocks=(0, 1, 2)):
        source = (x + dx) % 4
        if dx == 3:
            c_landing(0, 1).wait_recv()
        if dx == 1:
            c_landing(1, 0).wait_recv()
        for b in blocks:
            if dx == 2:
                for way, part in (((2, 0),), ((3, 0),), ((2, 1), (3, 1)))[b]:
                    c_pass(way, part, source).wait_recv()
            buffer, _ = staged(dx, b)
            base = ((3 * dx + b) % 4) * OUT_PART

            @pl.loop(0, OUT_PART // 256)
            def _(t):
                cols = pl.ds(pl.multiple_of(t * 256, 256), 256)
                to = pl.ds(pl.multiple_of(base + t * 256, 256), 256)
                if dx:
                    block = tokens[source, b // 2, :, (b % 2) * CONV : (b % 2 + 1) * CONV]
                else:
                    block = gated[b * BLOCK : (b + 1) * BLOCK, :]
                slots[buffer, :, to] = jnp.dot(block, w_conv[:, cols], preferred_element_type=F32).astype(BF16)

            conv_store(dx, b).start()

    def all_y_left():
        for dz in range(1, 4):
            for i in range(2):
                y_left(dz, i)

    def drain():
        for dz in (1, 2, 3):
            meta_copies[dz].wait_send()
        halo.wait_send()
        for g in range(4):
            sent = hidden.at[g, pl.ds(0, 3)]
            remote(sent, sent, h_send.at[g], h_recv.at[g, 0], at(0, 0, 0, 1)).wait_send()
            if g >= 2:
                b_left(g)
            for i in range(2):
                x_left(g, i)
        for way in range(2):
            c_left(way, ROWS)
        for dx in (0, 1, 3):
            conv_stored(dx)

    def finish():
        for dz in (1, 2, 3):
            p_left(dz)
        for way in (2, 3):
            c_left(way, ROWS // 2)
        pltpu.make_async_copy(out, out_hbm, out_sem).wait()
        conv_stored(2)

    def build_pair(number):
        for dz, i in PAIRS[number]:
            if number:
                take_z(dz, i)
            if number == 1:
                z_copy(2, i).start()
        if number == 1:
            meta_copies[1].wait_recv()
            meta_copies[3].wait_recv()
        if number == 3:
            meta_copies[2].wait_recv()
        for dz, i in PAIRS[number]:
            build(dz, i)
        send_slots(PAIRS[number])

    def pass_pair(number, between):
        pass_on(PAIRS[number], between)

    def wait_weights():
        for load in weights:
            load.wait()

    build_pair(0)
    conv_gate()
    conv_work = {0: [], 1: [take_halo]}
    for b in range(3):
        conv_work.setdefault(2 * b + 1, []).append(lambda b=b: conv_columns(b, 0))
        conv_work.setdefault(2 * b + 2, []).append(lambda b=b: conv_columns(b, 1))
        conv_work[2 * b + 2].append(lambda b=b: conv_norm(b))
    pass_pair(0, conv_work)
    build_pair(1)
    pass_pair(1, {3: [wait_weights, lambda: first_product(0)]})
    build_pair(2)
    pass_pair(2, {5: [lambda: build_pair(3)]})
    pass_pair(
        3,
        {
            0: [lambda: pass_hidden(0)],
            1: [lambda: first_product(1)],
            2: [lambda: first_product(3)],
            4: [lambda: pass_hidden(1), lambda: second_product(0)],
            5: [lambda: pass_hidden(3)],
        },
    )
    free_tokens()
    second_product(1)
    second_product(3)
    combine(0)
    first_product(2)
    combine(1)
    pass_hidden(2)
    conv_send()
    second_product(2)
    combine(3)
    combine(2)
    all_y_left()
    conv_pass()
    conv_product(0)
    conv_product(3)
    conv_product(1)
    drain()
    conv_product(2, (0, 1))
    final_sum()
    conv_product(2, (2,))
    finish()


def both_branches(*operands):
    vmem, hbm = pl.BlockSpec(memory_space=pltpu.VMEM), pl.BlockSpec(memory_space=pl.ANY)
    dma = pltpu.SemaphoreType.DMA
    return pl.pallas_call(
        kernel,
        name="experts",
        out_shape=(
            jax.ShapeDtypeStruct((4 * ROWS, OUT_PART), BF16),
            jax.ShapeDtypeStruct((512, OUT_PART), BF16),
        ),
        in_specs=[hbm, hbm, vmem, vmem, vmem, hbm, hbm, vmem, vmem, vmem, vmem, hbm, hbm, hbm],
        out_specs=(hbm, hbm),
        scratch_shapes=[
            pltpu.VMEM((4, 2, 128, D), BF16),
            pltpu.VMEM((6, 128, D), BF16),
            pltpu.VMEM((4, 8, 4, CAP, D), BF16),
            pltpu.VMEM((D, HID_PART), BF16),
            pltpu.VMEM((D, HID_PART), BF16),
            pltpu.VMEM((1024, OUT_PART), BF16),
            pltpu.VMEM((4, 4, 512, HID_PART), BF16),
            pltpu.VMEM((2, 8, 4, CAP, OUT_PART), BF16),
            pltpu.VMEM((4, 4, 8, CAP, OUT_PART), BF16),
            pltpu.VMEM((3, 512, OUT_PART), BF16),
            pltpu.VMEM((3, 512, OUT_PART), BF16),
            pltpu.VMEM((512, OUT_PART), BF16),
            pltpu.VMEM((4, 4, 8, 128), F32),
            pltpu.VMEM((512, HID_PART), F32),
            pltpu.VMEM((512, HID_PART), F32),
            pltpu.VMEM((HALO + ROWS, CONV), BF16),
            pltpu.VMEM((BLOCK, CONV), F32),
            pltpu.VMEM((CONV, OUT_PART), BF16),
            dma((10,)),
            dma((4, 2)),
            dma((4, 2)),
            dma((4,)),
            dma((4,)),
            dma((4, 2)),
            dma((4, 2, 8)),
            dma((4, 2)),
            dma((4, 2)),
            dma((4,)),
            dma((4, 4)),
            dma((4,)),
            dma((4, 2)),
            dma((4,)),
            dma((4, 2)),
            dma((2,)),
            dma((4,)),
            dma((4, 3)),
            dma((4,)),
            dma(()),
            pltpu.SemaphoreType.REGULAR,
        ],
        compiler_params=pltpu.CompilerParams(
            collective_id=0, has_side_effects=True, vmem_limit_bytes=67_043_328
        ),
        cost_estimate=pl.CostEstimate(flops=150_000_000_000, bytes_accessed=16 << 20, transcendentals=0),
    )(*operands)


def on_device(
    conv_value,
    conv_gate,
    conv_taps,
    conv_gain,
    conv_bias,
    conv_projection,
    expert_input,
    expert_gain,
    route_experts,
    group_gate,
    expert_gate,
    gate_weight,
    up_weight,
    down_weight,
):
    return both_branches(
        conv_value,
        conv_gate,
        conv_taps,
        conv_gain[None],
        conv_bias[None],
        conv_projection,
        expert_input,
        expert_gain[None],
        route_experts.T,
        group_gate[None],
        expert_gate.T,
        gate_weight,
        up_weight,
        down_weight,
    )


def solution(mesh):
    in_specs = (
        P(EP_TP, None),
        P(EP_TP, None),
        P(),
        P(),
        P(),
        P(None, "tp"),
        P("ep", None),
        P(),
        P("ep", None),
        P("ep"),
        P("ep", None),
        P("ep", None, "tp"),
        P("ep", None, "tp"),
        P("ep", None, "tp"),
    )
    out_specs = (P("ep", "tp"), P("ep", "tp"))
    return jax.shard_map(
        on_device, mesh=mesh, in_specs=in_specs, out_specs=out_specs, check_vma=False
    )
```

```python
import jax
import jax.numpy as jnp
from jax import lax
from jax.experimental import pallas as pl
from jax.experimental.pallas import tpu as pltpu
from jax.sharding import PartitionSpec as P

EXPERTS = 32
TOP = 2
MOE_DEV = 128
CAP = 16
D = 4096
CONV = 2048
KERNEL = 31
ROWS = 384
HALO = 32
BLOCK = 128
HID_PART = 256
OUT_PART = 1024
EP_TP = ("ep", "tp")
MESH = pl.DeviceIdType.MESH
BF16 = jnp.bfloat16
F32 = jnp.float32

epsilon = 1e-06

BUFFER = {(0, 0): 0, (0, 1): 1, (1, 0): 2, (3, 1): 3, (1, 1): 4, (3, 0): 5, (2, 0): 0, (2, 1): 1}
RESULT = {0: 0, 1: 1, 3: 0, 2: 1}
PAIRS = [((0, 0), (0, 1)), ((1, 0), (3, 1)), ((3, 0), (1, 1)), ((2, 0), (2, 1))]
Y_ORDER = [(0, 1), (1, 0), (3, 0), (1, 1), (3, 1), (2, 0), (2, 1)]


def kernel(
    value_hbm,
    gate_rows_hbm,
    taps,
    conv_gain,
    conv_bias,
    projection_hbm,
    rows_hbm,
    gain,
    route,
    group_gate,
    expert_gate,
    gate_hbm,
    up_hbm,
    down_hbm,
    conv_out,
    out_hbm,
    tokens,
    slots,
    arrived,
    w_gate,
    w_up,
    w_down,
    hidden,
    result,
    back,
    partial,
    landed,
    out,
    meta,
    acc_gate,
    acc_up,
    gated,
    mixed,
    w_conv,
    load_sem,
    z_send,
    z_recv,
    m_send,
    m_recv,
    y_send,
    y_recv,
    x_send,
    x_recv,
    h_send,
    h_recv,
    b_send,
    b_recv,
    p_send,
    p_recv,
    halo_sem,
    c_send,
    c_recv,
    store_sem,
    out_sem,
    free_sem,
):
    ep = lax.axis_index("ep")
    x = lax.axis_index("tp")
    z, y, c = ep // 8, (ep // 2) % 4, ep % 2

    def at(dz, dy, dc, dx):
        there = (((z + dz) % 4) * 4 + (y + dy) % 4) * 2 + (c + dc) % 2
        return (there, (x + dx) % 4)

    def remote(src, dst, send, recv, device):
        return pltpu.make_async_remote_copy(
            src_ref=src, dst_ref=dst, send_sem=send, recv_sem=recv, device_id=device, device_id_type=MESH
        )

    quarter = (x, (x + 1) % 4)
    number = ep * 4 + x
    after, ahead = (number + 1) % 128, (number + 127) % 128

    raw = [
        pltpu.make_async_copy(
            rows_hbm.at[pl.ds(pl.multiple_of(quarter[i] * MOE_DEV, MOE_DEV), MOE_DEV)],
            slots.at[2 + i],
            load_sem.at[i],
        )
        for i in range(2)
    ]
    value_load = pltpu.make_async_copy(value_hbm, gated.at[pl.ds(HALO, ROWS)], load_sem.at[2])
    gate_loads = [
        pltpu.make_async_copy(
            gate_rows_hbm.at[pl.ds(b * BLOCK, BLOCK)],
            slots.at[4 + b // 2, :, pl.ds((b % 2) * CONV, CONV)],
            load_sem.at[3 + b],
        )
        for b in range(3)
    ]
    weights = [
        pltpu.make_async_copy(gate_hbm.at[0], w_gate, load_sem.at[6]),
        pltpu.make_async_copy(up_hbm.at[0], w_up, load_sem.at[7]),
        pltpu.make_async_copy(down_hbm.at[0], w_down, load_sem.at[8]),
        pltpu.make_async_copy(projection_hbm, w_conv, load_sem.at[9]),
    ]
    for load in raw + [value_load] + gate_loads + weights:
        load.start()

    barrier = pltpu.get_barrier_semaphore()
    partners = [at(dz, 0, 0, 0) for dz in (1, 2, 3)]
    partners += [at(0, dy, dc, 0) for dy in range(4) for dc in range(2) if dy or dc]
    partners += [at(0, 0, 0, dx) for dx in (1, 2, 3)]
    partners += [(after // 4, after % 4), (ahead // 4, ahead % 4)]
    for device in partners:
        pl.semaphore_signal(barrier, inc=1, device_id=device, device_id_type=MESH)

    lane = lax.broadcasted_iota(jnp.int32, (128, 128), 1)
    sub = lax.broadcasted_iota(jnp.int32, (128, 128), 0)
    earlier = jnp.where(sub < lane, 1.0, 0.0).astype(BF16)
    expert_row = lax.broadcasted_iota(jnp.int32, (EXPERTS, 128), 0)
    for q in range(4):
        lanes = slice(q * MOE_DEV, (q + 1) * MOE_DEV)
        first, second = route[0:1, lanes], route[1:2, lanes]
        gates = expert_gate[:, lanes]
        hot0 = jnp.where(expert_row == first, 1.0, 0.0)
        hot1 = jnp.where(expert_row == second, 1.0, 0.0)
        before = jnp.dot((hot0 + hot1).astype(BF16), earlier, preferred_element_type=F32)
        pos0 = jnp.sum(before * hot0, axis=0, keepdims=True)
        pos1 = jnp.sum(before * hot1, axis=0, keepdims=True)
        meta[0, q, 0:1, :] = first.astype(F32) * CAP + pos0
        meta[0, q, 1:2, :] = second.astype(F32) * CAP + pos1
        meta[0, q, 2:4, :] = group_gate[:, lanes] * gates / jnp.sum(gates, axis=0, keepdims=True)
        meta[0, q, 4:8, :] = jnp.zeros((4, 128), F32)

    for i in range(2):
        raw[i].wait()

        @pl.loop(0, 8)
        def _(t):
            r = pl.ds(pl.multiple_of(t * 16, 16), 16)
            wide = slots[2 + i, r, :].astype(F32)
            inverse = lax.rsqrt(jnp.mean(wide * wide, axis=-1, keepdims=True) + epsilon)
            tokens[0, i, r, :] = (wide * inverse * gain[...]).astype(BF16)

    pl.semaphore_wait(barrier, len(partners))

    meta_copies = {
        dz: remote(meta.at[0], meta.at[dz], m_send.at[dz], m_recv.at[dz], at(dz, 0, 0, 0)) for dz in (1, 2, 3)
    }
    for dz in (1, 3, 2):
        meta_copies[dz].start()

    def z_copy(dz, i):
        if dz == 2:
            source, step = (1, 1) if i == 0 else (3, 3)
        else:
            source, step = 0, dz
        return remote(tokens.at[source, i], tokens.at[dz, i], z_send.at[dz, i], z_recv.at[dz, i], at(step, 0, 0, 0))

    for dz, i in ((1, 0), (3, 1), (1, 1), (3, 0)):
        z_copy(dz, i).start()

    plane = (z * 128).astype(F32)
    slot_row = lax.broadcasted_iota(jnp.int32, (128, 128), 0).astype(F32)

    def y_copy(dz, i, dy, dc):
        there = ((y + dy) % 4) * 2 + (c + dc) % 2
        k = dy * 2 + dc
        return remote(
            slots.at[BUFFER[dz, i], pl.ds(pl.multiple_of(there * CAP, CAP), CAP)],
            arrived.at[dz, k, quarter[i]],
            y_send.at[dz, i],
            y_recv.at[dz, i, k],
            at(0, dy, dc, 0),
        )

    def y_left(dz, i):
        sent = slots.at[BUFFER[dz, i], pl.ds(0, 7 * CAP)]
        remote(sent, sent, y_send.at[dz, i], y_recv.at[dz, i, 0], at(0, 1, 0, 0)).wait_send()

    def build(dz, i):
        q = quarter[i]
        if dz == 2:
            y_left(0, i)
        hot = jnp.where(slot_row == meta[dz, q, 0:1, :] - plane, 1.0, 0.0)
        hot = hot + jnp.where(slot_row == meta[dz, q, 1:2, :] - plane, 1.0, 0.0)
        hot = hot.astype(BF16)

        @pl.loop(0, D // 512)
        def _(t):
            cols = pl.ds(pl.multiple_of(t * 512, 512), 512)
            slots[BUFFER[dz, i], :, cols] = jnp.dot(
                hot, tokens[dz, i, :, cols], preferred_element_type=F32
            ).astype(BF16)


    def send_slots(pair):
        for dy, dc in Y_ORDER:
            for dz, i in pair:
                y_copy(dz, i, dy, dc).start()
        own = pl.ds(pl.multiple_of((y * 2 + c) * CAP, CAP), CAP)
        for dz, i in pair:
            arrived[dz, 0, quarter[i]] = slots[BUFFER[dz, i], own, :]

    def take_z(dz, i):
        z_copy(dz, i).wait_recv()

    def x_copy(dz, i, k):
        q = quarter[i]
        return remote(
            arrived.at[dz, k, q],
            arrived.at[dz, k, q],
            x_send.at[dz, i],
            x_recv.at[dz, i],
            at(0, 0, 0, 1 if i == 0 else 3),
        )

    def pass_on(pair, between):
        for dz, i in pair:
            x_copy(dz, i, 0).start()
        for step, (dy, dc) in enumerate(Y_ORDER):
            for work in between.get(step, ()):
                work()
            for dz, i in pair:
                y_copy(dz, i, dy, dc).wait_recv()
                x_copy(dz, i, dy * 2 + dc).start()

    def x_all(dz, i, q):
        place = arrived.at[dz, :, q]
        return remote(place, place, x_send.at[dz, i], x_recv.at[dz, i], at(0, 0, 0, 3 if i == 0 else 1))

    def x_landed(dz, i):
        x_all(dz, i, (x + 3) % 4 if i == 0 else (x + 2) % 4).wait_recv()

    def x_left(dz, i):
        x_all(dz, i, quarter[i]).wait_send()

    def h_copy(g, way, source):
        if g == 2 and way == 2:
            piece = hidden.at[g, source]
            return remote(piece, piece, h_send.at[g], h_recv.at[g, way], at(0, 0, 0, 2))
        half = pl.ds(0, 512) if way < 2 else pl.ds((way - 2) * 256, 256)
        piece = hidden.at[g, source, half]
        return remote(
            piece, piece, h_send.at[g], h_recv.at[g, way], at(0, 0, 0, 1 if way % 2 == 0 else 3)
        )

    KB = 512

    def first_product(g):
        for i in range(2):
            x_landed(g, i)
        acc_gate[...] = jnp.zeros_like(acc_gate)
        acc_up[...] = jnp.zeros_like(acc_up)

        @pl.loop(0, D // KB)
        def _(t):
            cols = pl.ds(pl.multiple_of(t * KB, KB), KB)
            piece = arrived[g, :, :, :, cols].reshape(512, KB)
            acc_gate[...] += jnp.dot(piece, w_gate[cols, :], preferred_element_type=F32)
            acc_up[...] += jnp.dot(piece, w_up[cols, :], preferred_element_type=F32)

        @pl.loop(0, 8)
        def _(t):
            r = pl.ds(pl.multiple_of(t * 64, 64), 64)
            gate = acc_gate[r, :]
            hidden[g, x, r, :] = (gate / (1.0 + jnp.exp(-gate)) * acc_up[r, :]).astype(BF16)

        for way in (0, 1, 2) if g == 2 else (0, 1):
            h_copy(g, way, x).start()

    def pass_hidden(g):
        h_copy(g, 0, (x + 3) % 4).wait_recv()
        if g != 2:
            h_copy(g, 2, (x + 3) % 4).start()
        h_copy(g, 1, (x + 1) % 4).wait_recv()
        if g != 2:
            h_copy(g, 3, (x + 1) % 4).start()

    def b_copy(g, dy, dc, half):
        pick = pl.ds(half * 2, 2)
        return remote(
            result.at[RESULT[g], dy * 2 + dc, pick],
            back.at[g, pick, y * 2 + c],
            b_send.at[g],
            b_recv.at[g, half],
            at(0, (4 - dy) % 4, dc, 0),
        )

    def b_left(g):
        sent = result.at[RESULT[g], pl.ds(1, 7)]
        remote(sent, sent, b_send.at[g], b_recv.at[g, 0], at(0, 1, 0, 0)).wait_send()

    def b_landed(g, half):
        place = result.at[RESULT[g], pl.ds(1, 7), pl.ds(0, 2)]
        remote(place, place, b_send.at[g], b_recv.at[g, half], at(0, 1, 0, 0)).wait_recv()

    def second_product(g):
        for way in (2,) if g == 2 else (2, 3):
            h_copy(g, way, (x + 2) % 4).wait_recv()
        if g >= 2:
            b_left(0 if g == 3 else 1)

        @pl.loop(0, OUT_PART // 256)
        def _(t):
            cols = pl.ds(pl.multiple_of(t * 256, 256), 256)
            total = jnp.dot(hidden[g, 0], w_down[0:256, cols], preferred_element_type=F32)
            for s in range(1, 4):
                total += jnp.dot(hidden[g, s], w_down[s * 256 : (s + 1) * 256, cols], preferred_element_type=F32)
            result[RESULT[g], :, :, :, cols] = total.astype(BF16).reshape(8, 4, CAP, 256)

        for half in range(2):
            for dy, dc in Y_ORDER:
                b_copy(g, dy, dc, half).start()
        back[g, :, y * 2 + c] = result[RESULT[g], 0]

    def p_copy(g, half):
        r = pl.ds(half * 256, 256)
        return remote(
            partial.at[g - 1, r], landed.at[g - 1, r], p_send.at[g], p_recv.at[g, half], at(4 - g, 0, 0, 0)
        )

    def p_left(g):
        sent = partial.at[g - 1]
        remote(sent, sent, p_send.at[g], p_recv.at[g, 0], at(1, 0, 0, 0)).wait_send()

    def combine(g):
        for half in range(2):
            b_landed(g, half)

            @pl.loop(half * 2, half * 2 + 2)
            def _(q):
                weight = jnp.where(slot_row == meta[g, q, 0:1, :] - plane, meta[g, q, 2:3, :], 0.0)
                weight = weight + jnp.where(slot_row == meta[g, q, 1:2, :] - plane, meta[g, q, 3:4, :], 0.0)
                high = weight.astype(BF16)
                low = (weight - high.astype(F32)).astype(BF16)
                rows = back[g, q].reshape(128, OUT_PART)
                dims = (((0,), (0,)), ((), ()))
                total = lax.dot_general(high, rows, dims, preferred_element_type=F32)
                total += lax.dot_general(low, rows, dims, preferred_element_type=F32)
                r = pl.ds(pl.multiple_of(q * 128, 128), 128)
                if g:
                    partial[g - 1, r, :] = total.astype(BF16)
                else:
                    out[r, :] = total.astype(BF16)

            if g:
                p_copy(g, half).start()

    def out_store(part):
        r = pl.ds(part * 128, 128)
        return pltpu.make_async_copy(out.at[r], out_hbm.at[r], out_sem)

    def final_sum():
        for part in range(4):
            if part % 2 == 0:
                for g in (1, 3, 2):
                    p_copy(g, part // 2).wait_recv()

            @pl.loop(0, 4)
            def _(t):
                r = pl.ds(pl.multiple_of(part * 128 + t * 32, 32), 32)
                total = out[r, :].astype(F32) + landed[0, r, :].astype(F32)
                total = total + landed[1, r, :].astype(F32) + landed[2, r, :].astype(F32)
                out[r, :] = total.astype(BF16)

            out_store(part).start()

    halo = remote(
        gated.at[pl.ds(ROWS, HALO)], gated.at[pl.ds(0, HALO)], halo_sem.at[0], halo_sem.at[1], (after // 4, after % 4)
    )

    def conv_gate():
        value_load.wait()
        for load in gate_loads:
            load.wait()
        for b in range(3):

            @pl.loop(0, BLOCK // 16)
            def _(t):
                r = pl.ds(pl.multiple_of(t * 16, 16), 16)
                to = pl.ds(pl.multiple_of(HALO + b * BLOCK + t * 16, 16), 16)
                gate = slots[4 + b // 2, r, (b % 2) * CONV : (b % 2 + 1) * CONV].astype(F32)
                gated[to, :] = (gated[to, :].astype(F32) / (1.0 + jnp.exp(-gate))).astype(BF16)

        halo.start()

    tile_row = lax.broadcasted_iota(jnp.int32, (8, 128), 0)

    def take_halo():
        halo.wait_recv()

        @pl.when(number == 0)
        def _():
            gated[0:HALO, :] = jnp.zeros((HALO, CONV), BF16)

    def conv_columns(b, half):
        @pl.loop(half * (CONV // 256), (half + 1) * (CONV // 256))
        def _(t):
            cols = pl.ds(pl.multiple_of(t * 128, 128), 128)
            tap = [jnp.broadcast_to(taps[j : j + 1, cols], (8, 128)) for j in range(KERNEL)]
            tiles = []
            last = None
            for n in range((HALO + BLOCK) // 16):
                pair = gated[b * BLOCK + n * 16 : b * BLOCK + (n + 1) * 16, cols].astype(F32)
                for half in (pair[0:8], pair[8:16]):
                    tiles.append(half)
                    count = len(tiles)
                    if count < 4:
                        continue
                    sums = []
                    for j in range(8):
                        total = tap[j] * tiles[count - 1]
                        for a in range(1, 4):
                            if 8 * a + j < KERNEL:
                                total = total + tap[8 * a + j] * tiles[count - 1 - a]
                        sums.append(total)
                    if count > 4:
                        total = sums[0]
                        for j in range(1, 8):
                            total = total + pltpu.roll(jnp.where(tile_row >= 8 - j, last[j], sums[j]), j, 0)
                        row = (count - 5) * 8
                        mixed[row : row + 8, cols] = total
                    last = sums

    def conv_norm(b):
        @pl.loop(0, BLOCK // 16)
        def _(t):
            r = pl.ds(pl.multiple_of(t * 16, 16), 16)
            wide = mixed[r, :]
            center = wide - jnp.mean(wide, axis=-1, keepdims=True)
            spread = jnp.mean(center * center, axis=-1, keepdims=True)
            unit = center * lax.rsqrt(spread + epsilon) * conv_gain[...] + conv_bias[...]
            to = pl.ds(pl.multiple_of(b * BLOCK + t * 16, 16), 16)
            gated[to, :] = (unit / (1.0 + jnp.exp(-unit))).astype(BF16)

    def held(source, b, start=0, rows=BLOCK):
        return tokens.at[source, b // 2, pl.ds(start, rows), pl.ds((b % 2) * CONV, CONV)]

    def c_copy(way, b):
        return remote(
            gated.at[pl.ds(b * BLOCK, BLOCK)],
            held(x, b),
            c_send.at[way],
            c_recv.at[way, b],
            at(0, 0, 0, 1 if way == 0 else 3),
        )

    def c_landing(way, b):
        place = held((x + 3) % 4 if way == 0 else (x + 1) % 4, b)
        return remote(place, place, c_send.at[way], c_recv.at[way, b], at(0, 0, 0, 1 if way == 0 else 3))

    def c_pass(way, part, source):
        place = held(source, way - 2) if part == 0 else held(source, 2, (way - 2) * 64, 64)
        return remote(place, place, c_send.at[way], c_recv.at[way, part], at(0, 0, 0, 1 if way == 2 else 3))

    def c_left(way, rows):
        sent = gated.at[pl.ds(0, rows)]
        remote(sent, sent, c_send.at[way], c_recv.at[way, 0], at(0, 0, 0, 1)).wait_send()

    def free_tokens():
        for dz in (1, 2, 3):
            for i in range(2):
                z_copy(dz, i).wait_send()
        for dx in (1, 2, 3):
            pl.semaphore_signal(free_sem, inc=1, device_id=at(0, 0, 0, dx), device_id_type=MESH)

    def conv_send():
        pl.semaphore_wait(free_sem, 3)
        for turn in range(3):
            for way in range(2):
                c_copy(way, ((0, 2, 1), (1, 2, 0))[way][turn]).start()

    def conv_pass():
        c_landing(0, 0).wait_recv()
        c_pass(2, 0, (x + 3) % 4).start()
        c_landing(1, 1).wait_recv()
        c_pass(3, 0, (x + 1) % 4).start()
        c_landing(0, 2).wait_recv()
        c_pass(2, 1, (x + 3) % 4).start()
        c_landing(1, 2).wait_recv()
        c_pass(3, 1, (x + 1) % 4).start()

    def staged(dx, b):
        n = 3 * dx + b
        return n // 4, pl.ds((n % 4) * OUT_PART, OUT_PART)

    def conv_store(dx, b):
        source = (x + dx) % 4
        buffer, cols = staged(dx, b)
        return pltpu.make_async_copy(
            slots.at[buffer, :, cols],
            conv_out.at[pl.ds(pl.multiple_of(source * ROWS + b * BLOCK, BLOCK), BLOCK)],
            store_sem.at[dx],
        )

    def conv_stored(dx):
        rows = conv_out.at[pl.ds(0, ROWS)]
        pltpu.make_async_copy(rows, rows, store_sem.at[dx]).wait()

    def conv_product(dx, blocks=(0, 1, 2)):
        source = (x + dx) % 4
        if dx == 3:
            c_landing(0, 1).wait_recv()
        if dx == 1:
            c_landing(1, 0).wait_recv()
        for b in blocks:
            if dx == 2:
                for way, part in (((2, 0),), ((3, 0),), ((2, 1), (3, 1)))[b]:
                    c_pass(way, part, source).wait_recv()
            buffer, _ = staged(dx, b)
            base = ((3 * dx + b) % 4) * OUT_PART

            @pl.loop(0, OUT_PART // 256)
            def _(t):
                cols = pl.ds(pl.multiple_of(t * 256, 256), 256)
                to = pl.ds(pl.multiple_of(base + t * 256, 256), 256)
                if dx:
                    block = tokens[source, b // 2, :, (b % 2) * CONV : (b % 2 + 1) * CONV]
                else:
                    block = gated[b * BLOCK : (b + 1) * BLOCK, :]
                slots[buffer, :, to] = jnp.dot(block, w_conv[:, cols], preferred_element_type=F32).astype(BF16)

            conv_store(dx, b).start()

    def all_y_left():
        for dz in range(1, 4):
            for i in range(2):
                y_left(dz, i)

    def drain():
        for dz in (1, 2, 3):
            meta_copies[dz].wait_send()
        halo.wait_send()
        for g in range(4):
            sent = hidden.at[g, pl.ds(0, 3)]
            remote(sent, sent, h_send.at[g], h_recv.at[g, 0], at(0, 0, 0, 1)).wait_send()
            if g >= 2:
                b_left(g)
            for i in range(2):
                x_left(g, i)
        for way in range(2):
            c_left(way, ROWS)
        for dx in (0, 1, 3):
            conv_stored(dx)

    def finish():
        for dz in (1, 2, 3):
            p_left(dz)
        for way in (2, 3):
            c_left(way, ROWS // 2)
        pltpu.make_async_copy(out, out_hbm, out_sem).wait()
        conv_stored(2)

    def build_pair(number):
        for dz, i in PAIRS[number]:
            if number:
                take_z(dz, i)
            if number == 1:
                z_copy(2, i).start()
        if number == 1:
            meta_copies[1].wait_recv()
            meta_copies[3].wait_recv()
        if number == 3:
            meta_copies[2].wait_recv()
        for dz, i in PAIRS[number]:
            build(dz, i)
        send_slots(PAIRS[number])

    def pass_pair(number, between):
        pass_on(PAIRS[number], between)

    def wait_weights():
        for load in weights:
            load.wait()

    build_pair(0)
    conv_gate()
    conv_work = {0: [], 1: [take_halo]}
    for b in range(3):
        conv_work.setdefault(2 * b + 1, []).append(lambda b=b: conv_columns(b, 0))
        conv_work.setdefault(2 * b + 2, []).append(lambda b=b: conv_columns(b, 1))
        conv_work[2 * b + 2].append(lambda b=b: conv_norm(b))
    pass_pair(0, conv_work)
    build_pair(1)
    pass_pair(1, {3: [wait_weights, lambda: first_product(0)]})
    build_pair(2)
    pass_pair(2, {5: [lambda: build_pair(3)]})
    pass_pair(
        3,
        {
            0: [lambda: pass_hidden(0)],
            1: [lambda: first_product(1)],
            2: [lambda: first_product(3)],
            4: [lambda: pass_hidden(1), lambda: second_product(0)],
            5: [lambda: pass_hidden(3)],
        },
    )
    free_tokens()
    second_product(1)
    second_product(3)
    combine(0)
    first_product(2)
    conv_send()
    combine(1)
    pass_hidden(2)
    second_product(2)
    combine(3)
    combine(2)
    all_y_left()
    conv_pass()
    conv_product(0)
    conv_product(3)
    conv_product(1)
    drain()
    conv_product(2, (0, 1))
    final_sum()
    conv_product(2, (2,))
    finish()


def both_branches(*operands):
    vmem, hbm = pl.BlockSpec(memory_space=pltpu.VMEM), pl.BlockSpec(memory_space=pl.ANY)
    dma = pltpu.SemaphoreType.DMA
    return pl.pallas_call(
        kernel,
        name="experts",
        out_shape=(
            jax.ShapeDtypeStruct((4 * ROWS, OUT_PART), BF16),
            jax.ShapeDtypeStruct((512, OUT_PART), BF16),
        ),
        in_specs=[hbm, hbm, vmem, vmem, vmem, hbm, hbm, vmem, vmem, vmem, vmem, hbm, hbm, hbm],
        out_specs=(hbm, hbm),
        scratch_shapes=[
            pltpu.VMEM((4, 2, 128, D), BF16),
            pltpu.VMEM((6, 128, D), BF16),
            pltpu.VMEM((4, 8, 4, CAP, D), BF16),
            pltpu.VMEM((D, HID_PART), BF16),
            pltpu.VMEM((D, HID_PART), BF16),
            pltpu.VMEM((1024, OUT_PART), BF16),
            pltpu.VMEM((4, 4, 512, HID_PART), BF16),
            pltpu.VMEM((2, 8, 4, CAP, OUT_PART), BF16),
            pltpu.VMEM((4, 4, 8, CAP, OUT_PART), BF16),
            pltpu.VMEM((3, 512, OUT_PART), BF16),
            pltpu.VMEM((3, 512, OUT_PART), BF16),
            pltpu.VMEM((512, OUT_PART), BF16),
            pltpu.VMEM((4, 4, 8, 128), F32),
            pltpu.VMEM((512, HID_PART), F32),
            pltpu.VMEM((512, HID_PART), F32),
            pltpu.VMEM((HALO + ROWS, CONV), BF16),
            pltpu.VMEM((BLOCK, CONV), F32),
            pltpu.VMEM((CONV, OUT_PART), BF16),
            dma((10,)),
            dma((4, 2)),
            dma((4, 2)),
            dma((4,)),
            dma((4,)),
            dma((4, 2)),
            dma((4, 2, 8)),
            dma((4, 2)),
            dma((4, 2)),
            dma((4,)),
            dma((4, 4)),
            dma((4,)),
            dma((4, 2)),
            dma((4,)),
            dma((4, 2)),
            dma((2,)),
            dma((4,)),
            dma((4, 3)),
            dma((4,)),
            dma(()),
            pltpu.SemaphoreType.REGULAR,
        ],
        compiler_params=pltpu.CompilerParams(
            collective_id=0, has_side_effects=True, vmem_limit_bytes=67_043_328
        ),
        cost_estimate=pl.CostEstimate(flops=150_000_000_000, bytes_accessed=16 << 20, transcendentals=0),
    )(*operands)


def on_device(
    conv_value,
    conv_gate,
    conv_taps,
    conv_gain,
    conv_bias,
    conv_projection,
    expert_input,
    expert_gain,
    route_experts,
    group_gate,
    expert_gate,
    gate_weight,
    up_weight,
    down_weight,
):
    return both_branches(
        conv_value,
        conv_gate,
        conv_taps,
        conv_gain[None],
        conv_bias[None],
        conv_projection,
        expert_input,
        expert_gain[None],
        route_experts.T,
        group_gate[None],
        expert_gate.T,
        gate_weight,
        up_weight,
        down_weight,
    )


def solution(mesh):
    in_specs = (
        P(EP_TP, None),
        P(EP_TP, None),
        P(),
        P(),
        P(),
        P(None, "tp"),
        P("ep", None),
        P(),
        P("ep", None),
        P("ep"),
        P("ep", None),
        P("ep", None, "tp"),
        P("ep", None, "tp"),
        P("ep", None, "tp"),
    )
    out_specs = (P("ep", "tp"), P("ep", "tp"))
    return jax.shard_map(
        on_device, mesh=mesh, in_specs=in_specs, out_specs=out_specs, check_vma=False
    )
```
